128 devices in a mesh: ep: 32 (over z, y, core), tp: 4 (over x).
Axes of the slice: x: 4, y: 4, z: 4, core: 2. Of those that a mesh axis runs over, the one named last changes fastest.
Arguments:
- tokens: bfloat16 [512, 2048], P('ep'), may hold values from -60 to 60
- mixer_gain: float32 [2048], replicated, may hold values from 0.1 to 1.9
- query_weight: bfloat16 [2048, 2048], P('ep', 'tp'), may hold values from -0.125 to 0.125
- key_weight: bfloat16 [2048, 2048], P('ep', 'tp'), may hold values from -0.125 to 0.125
- value_weight: bfloat16 [2048, 2048], P('ep', 'tp'), may hold values from -0.125 to 0.125
- outgate_weight: bfloat16 [2048, 2048], P('ep', 'tp'), may hold values from -0.125 to 0.125
- igate_weight: bfloat16 [4, 2048], P('tp'), may hold values from -0.125 to 0.125
- fgate_weight: bfloat16 [4, 2048], P('tp'), may hold values from -0.125 to 0.125
- memory: float32 [512, 4, 512, 512], P('ep', 'tp'), may hold values from -6 to 6
- stabilizer: float32 [512, 4], P('ep', 'tp'), may hold values from -6 to 6
- head_gain: float32 [2048], P('tp'), may hold values from 0.1 to 1.9
- down_weight: bfloat16 [2048, 2048], P(None, 'ep'), may hold values from -1 to 1
- mixed_gain: float32 [2048], P('ep'), may hold values from 0.1 to 1.9
- expert_gain: float32 [2048], P('ep'), may hold values from 0.1 to 1.9
- routes: int32 [512, 4], replicated, may hold values from 0 to 31, all different within a row; in each aligned block of 16 rows (0 to 15, 16 to 31, ...) at most 4 rows name the same one
- route_weights: float32 [512, 4], replicated, may hold values from 0.1 to 1
- gate_proj: bfloat16 [32, 2048, 2048], P('ep', None, 'tp'), may hold values from -0.5 to 0.5
- up_proj: bfloat16 [32, 2048, 2048], P('ep', None, 'tp'), may hold values from -0.5 to 0.5
- expert_down: bfloat16 [32, 2048, 2048], P('ep', 'tp'), may hold values from -1 to 1
- output_gain: float32 [2048], P('tp'), may hold values from 0.1 to 1.9
Outputs:
- layer_out: bfloat16 [512, 2048], P('ep', 'tp')
The draws below stay inside these ranges and needn't reach their ends.
Inputs may be any that keep to these rules, and one draw needn't show every extreme that they name: `routes`: each row names 4 different experts; within the rows of one device (16 rows) no expert is named more than 4 times, a bound that some block reaches.
All inputs are finite; a program needn't handle non-finite values.
Results may differ from the reference program's by a relative error of at most 0.0095.
Values may be sent and summed in bfloat16 or wider, within the bound.
A program may use at most 128 MiB of HBM per device.

```python
import math
import jax
import jax.numpy as jnp
import numpy as np
from jax import lax

D = 2048
HEADS = 4
DH = 512
DE = 2048
TOP_K = 4
SEQ_DEV = 16
TOKENS = 512
EXPERTS = 32
CAP = 4
N_EP = 32


def column_ramp(key, width, spread):
    rough = jax.random.uniform(key, (width,), jnp.float32, -0.3, 0.3)
    return jnp.exp(jnp.linspace(-spread, spread, width) + rough)


def draw_tokens(key, part):
    base = jax.random.normal(jax.random.fold_in(key, 11), (TOKENS, D), jnp.float32)
    row_scale = jnp.exp(jax.random.uniform(jax.random.fold_in(key, 12), (TOKENS, 1), jnp.float32, jnp.log(0.4), jnp.log(4.0)))
    ramp = column_ramp(jax.random.fold_in(key, 14), D, 0.55)
    values = base * row_scale * ramp[None, :]
    return jnp.clip(values, -60.0, 60.0).astype(jnp.bfloat16)


def draw_down_weight(key, part):
    base = jax.random.normal(jax.random.fold_in(key, 21), (HEADS * DH, D), jnp.float32) / jnp.sqrt(HEADS * DH * 1.0)
    ramp = column_ramp(jax.random.fold_in(key, 22), D, 0.55)
    return jnp.clip(base * ramp[None, :], -1.0, 1.0).astype(jnp.bfloat16)


def draw_expert_down(key, part):
    base = jax.random.normal(jax.random.fold_in(key, 31), (EXPERTS, DE, D), jnp.float32) / jnp.sqrt(DE * 1.0)
    ramp = column_ramp(jax.random.fold_in(key, 32), D, 0.55)
    return jnp.clip(base * ramp[None, None, :], -1.0, 1.0).astype(jnp.bfloat16)


def level_of(own_key, shape, shards, low, high):
    def one(dim, parts):
        draws = jax.random.uniform(jax.random.fold_in(jax.random.fold_in(own_key, 6), dim), (parts,), jnp.float32, low / len(shards), high / len(shards))
        return jnp.repeat(jnp.exp(draws), shape[dim] // parts).reshape((-1,) + (1,) * (len(shape) - dim - 1))

    loudness = one(*shards[0])
    for cut in shards[1:]:
        loudness = loudness * one(*cut)
    return loudness


def assign_block(stream_key, own, number, rows, amount, top, bound, skew):
    order = jax.random.permutation(stream_key, amount)
    crowded, usual = load_shares(amount, rows * top, bound, skew, True), load_shares(amount, rows * top, bound, skew, False)
    places = jnp.arange(amount)

    def named(lengths, rotation):
        used = int((lengths > 0).sum())
        fixed = max(1, used // 4)
        passed = fixed + (places - fixed + rotation * (used - fixed)) % max(1, amount - fixed)
        return jnp.zeros((amount,), jnp.int32).at[order[jnp.where(places < fixed, places, passed)]].set(jnp.asarray(lengths, jnp.int32))

    lengths = jnp.where(number % 4 == 0, named(crowded, number // 4), named(usual, number - number // 4 - 1))
    mixed = jax.random.permutation(jax.random.fold_in(own, 3), amount)
    donor, sink = mixed[0:amount // 2 * 2:2], mixed[1:amount // 2 * 2:2]
    slack = jnp.minimum(lengths[donor] - 1, bound - lengths[sink]) // 2
    slack = jnp.where((donor == order[0]) | (sink == order[0]) | (lengths[sink] == 0), 0, jnp.maximum(slack, 0))
    passed = jax.random.randint(jax.random.fold_in(own, 4), (amount // 2,), 0, 1 << 20) % (slack + 1)
    lengths = lengths.at[donor].add(-passed).at[sink].add(passed)
    members = jnp.searchsorted(jnp.cumsum(lengths), jnp.arange(rows * top), side="right").astype(jnp.int32)
    table = members.reshape(top, rows).T
    table = table[jax.random.permutation(jax.random.fold_in(own, 1), rows)]
    rotation = jax.random.randint(jax.random.fold_in(own, 2), (rows, 1), 0, top)
    return jnp.take_along_axis(table, (jnp.arange(top)[None, :] + rotation) % top, axis=1)


def load_shares(count, total, most, lean, full):
    loads = [(1 << 20) // math.isqrt(standing ** lean) + 1 for standing in range(1, count + 1)]
    largest = most if full else min(most, max(-(-total // count), total * loads[0] // sum(loads)))
    least = 1 if total - largest >= count - 1 else 0
    given, surplus = [largest] + [least] * (count - 1), total - largest - least * (count - 1)
    while surplus > 0:
        free = [i for i in range(1, count) if given[i] < largest] or [i for i in range(1, count) if given[i] < most]
        mass, budget = sum([loads[i] for i in free]), surplus
        for i in free:
            extra = min(most - given[i], max(1, budget * loads[i] // mass), surplus)
            given[i] = given[i] + extra
            surplus = surplus - extra
    return np.array(given)


def centred(key, shape, scale, reach, cuts=(), held_as=jnp.bfloat16):
    loudness = level_of(key, shape, cuts, -0.22, 0.18) if cuts else 1.0
    drawn = jax.random.normal(key, shape, jnp.float32) * scale * loudness
    return jnp.minimum(jnp.maximum(drawn, -reach), reach).astype(held_as)


def setup_inputs(seed: int = 0) -> dict:
    streams_of = jax.random.split(jax.random.key(seed), 21)
    tokens = draw_tokens(jax.random.fold_in(streams_of[20], 71), 0)
    mixer_gain = jnp.clip(1.0 + 0.18 * jax.random.normal(streams_of[1], (D,), jnp.float32), 0.1, 1.9)
    query_weight = centred(streams_of[2], (D, HEADS * DH), D ** -0.5, 0.125, ((0, 32), (1, 4)))
    key_weight = centred(streams_of[3], (D, HEADS * DH), D ** -0.5, 0.125, ((0, 32), (1, 4)))
    value_weight = centred(streams_of[4], (D, HEADS * DH), D ** -0.5, 0.125, ((0, 32), (1, 4)))
    outgate_weight = centred(streams_of[5], (D, HEADS * DH), D ** -0.5, 0.125, ((0, 32), (1, 4)))
    igate_weight = centred(streams_of[6], (HEADS, D), D ** -0.5, 0.125, ((0, 4),))
    fgate_weight = centred(streams_of[7], (HEADS, D), D ** -0.5, 0.125, ((0, 4),))
    memory = centred(streams_of[8], (TOKENS, HEADS, DH, DH), 1.0, 6.0, ((0, 32), (1, 4)), jnp.float32)
    stabilizer = centred(streams_of[9], (TOKENS, HEADS), 1.5, 6.0, ((0, 32), (1, 4)), jnp.float32)
    head_gain = jnp.clip(1.0 + 0.18 * jax.random.normal(streams_of[10], (HEADS * DH,), jnp.float32), 0.1, 1.9)
    down_weight = draw_down_weight(jax.random.fold_in(streams_of[20], 71), 0)
    mixed_gain = jnp.clip(1.0 + 0.18 * jax.random.normal(streams_of[12], (D,), jnp.float32), 0.1, 1.9)
    expert_gain = jnp.clip(1.0 + 0.18 * jax.random.normal(streams_of[13], (D,), jnp.float32), 0.1, 1.9)
    routes_keys = jax.random.split(jax.random.fold_in(streams_of[14], 1), TOKENS // SEQ_DEV)
    routes_turns = jax.random.permutation(jax.random.fold_in(streams_of[14], 3), TOKENS // SEQ_DEV)
    routes = jax.vmap(lambda own, number: assign_block(jax.random.fold_in(streams_of[14], 2), own, number, SEQ_DEV, EXPERTS, TOP_K, CAP, 2))(routes_keys, routes_turns).reshape((TOKENS, TOP_K))
    route_weights = jnp.clip(jax.random.uniform(streams_of[15], (TOKENS, TOP_K), jnp.float32, 0.1, 1.0), 0.1, 1.0)
    gate_proj = centred(streams_of[16], (EXPERTS, D, DE), (D // 16) ** -0.5, 0.5, ((0, 32), (2, 4)))
    up_proj = centred(streams_of[17], (EXPERTS, D, DE), (D // 16) ** -0.5, 0.5, ((0, 32), (2, 4)))
    expert_down = draw_expert_down(jax.random.fold_in(streams_of[20], 71), 0)
    output_gain = jnp.clip(1.0 + 0.18 * jax.random.normal(streams_of[19], (D,), jnp.float32), 0.1, 1.9)
    return dict(tokens=tokens, mixer_gain=mixer_gain, query_weight=query_weight, key_weight=key_weight, value_weight=value_weight, outgate_weight=outgate_weight, igate_weight=igate_weight, fgate_weight=fgate_weight, memory=memory, stabilizer=stabilizer, head_gain=head_gain, down_weight=down_weight, mixed_gain=mixed_gain, expert_gain=expert_gain, routes=routes, route_weights=route_weights, gate_proj=gate_proj, up_proj=up_proj, expert_down=expert_down, output_gain=output_gain)


NORM_EPS = 1e-06
CLAMP_LIMIT = 7.0
SIGMOID_SCALE = 1.702

def rms_scale(values):
    return lax.rsqrt(lax.optimization_barrier(jnp.mean(values * values, axis=-1, keepdims=True)) + NORM_EPS)

def slot_tables(routes, groups, experts, capacity):
    token_total, top_count = routes.shape
    per_group = token_total // groups
    flat_routes = routes.reshape(groups, per_group * top_count)
    onehot = (flat_routes[:, :, None] == jnp.arange(experts, dtype=jnp.int32)[None, None, :]).astype(jnp.int32)
    before = jnp.cumsum(onehot, axis=1) - onehot
    slot_index = lax.optimization_barrier(jnp.sum(before * onehot, axis=2))
    group_ids = jnp.arange(groups, dtype=jnp.int32)[:, None]
    destination = ((flat_routes * groups + group_ids) * capacity + slot_index).reshape(token_total, top_count)
    owner_token = jnp.arange(token_total * top_count, dtype=jnp.int32) // top_count
    slot_token = jnp.full((experts * groups * capacity,), token_total, jnp.int32).at[destination.reshape(-1)].set(owner_token)
    return (destination, slot_token)

def read_memory(projected, log_input, log_forget, memory, stabilizer, head_gain):
    row_total, head_count, head_size = (memory.shape[0], memory.shape[1], memory.shape[3])
    query_scaled = projected[:, 0] * head_size ** (-0.5)
    key_rows = projected[:, 1]
    value_rows = projected[:, 2]
    outgate_rows = projected[:, 3]
    peak_log = jnp.maximum(log_forget + stabilizer, log_input)
    within = jnp.exp(log_input - peak_log)
    carried = jnp.exp(log_forget + stabilizer - peak_log)
    scores = lax.optimization_barrier(jnp.sum(query_scaled * key_rows, axis=-1)) * within
    state_read = jnp.einsum('nhd,nhde->nhe', query_scaled, memory, precision=lax.Precision.HIGHEST)
    read_value = scores[..., None] * value_rows + carried[..., None] * state_read
    head_mean = lax.optimization_barrier(jnp.mean(read_value, axis=-1, keepdims=True))
    centered = read_value - head_mean
    head_var = lax.optimization_barrier(jnp.mean(centered * centered, axis=-1, keepdims=True))
    normalized = centered * lax.rsqrt(head_var + NORM_EPS)
    gained = normalized * head_gain.reshape(head_count, head_size) * jax.nn.sigmoid(outgate_rows)
    return gained.reshape(row_total, head_count * head_size).astype(jnp.bfloat16)

def apply_expert(arguments):
    row_block, gate_matrix, up_matrix, down_matrix = arguments
    gate_pre = jnp.minimum(jnp.dot(row_block, gate_matrix, preferred_element_type=jnp.float32), CLAMP_LIMIT)
    up_pre = jnp.clip(jnp.dot(row_block, up_matrix, preferred_element_type=jnp.float32), -CLAMP_LIMIT, CLAMP_LIMIT)
    activation = ((up_pre + 1.0) * gate_pre * jax.nn.sigmoid(SIGMOID_SCALE * gate_pre)).astype(jnp.bfloat16)
    return jnp.dot(activation, down_matrix, preferred_element_type=jnp.float32)

def reference(tokens, mixer_gain, query_weight, key_weight, value_weight, outgate_weight, igate_weight, fgate_weight, memory, stabilizer, head_gain, down_weight, mixed_gain, expert_gain, routes, route_weights, gate_proj, up_proj, expert_down, output_gain):
    tokens_float = tokens.astype(jnp.float32)
    normed = (tokens_float * rms_scale(tokens_float) * mixer_gain).astype(jnp.bfloat16)
    projected = jnp.concatenate([jnp.dot(normed, matrix, preferred_element_type=jnp.float32) for matrix in (query_weight, key_weight, value_weight, outgate_weight)], axis=1).astype(jnp.bfloat16)
    projected = lax.optimization_barrier(projected).astype(jnp.float32).reshape(TOKENS, 4, HEADS, DH)
    log_input = jnp.dot(normed, igate_weight.T, preferred_element_type=jnp.float32)
    log_forget = jax.nn.log_sigmoid(jnp.dot(normed, fgate_weight.T, preferred_element_type=jnp.float32))
    gated_heads = read_memory(projected, log_input, log_forget, memory, stabilizer, head_gain)
    mixed_rows = jnp.dot(gated_heads, down_weight, preferred_element_type=jnp.float32)
    residual_float = tokens_float + mixed_rows * rms_scale(mixed_rows) * mixed_gain
    residual = residual_float.astype(jnp.bfloat16)
    expert_in = (residual_float * rms_scale(residual_float) * expert_gain).astype(jnp.bfloat16)
    destination, slot_token = slot_tables(routes, N_EP, EXPERTS, CAP)
    padded_in = jnp.concatenate([expert_in, jnp.zeros((1, D), jnp.bfloat16)], axis=0)
    expert_inputs = padded_in[slot_token].reshape(EXPERTS, N_EP * CAP, D)
    expert_out = lax.map(apply_expert, (expert_inputs, gate_proj, up_proj, expert_down))
    picked = expert_out.reshape(EXPERTS * N_EP * CAP, D)[destination]
    combined = lax.optimization_barrier(jnp.sum(picked * route_weights[..., None], axis=1))
    final_rows = residual.astype(jnp.float32) + combined * rms_scale(combined) * output_gain
    return final_rows.astype(jnp.bfloat16)
```

```python
import functools
import jax
import jax.numpy as jnp
from jax import lax
from jax.experimental import pallas as pl
from jax.experimental.pallas import tpu as pltpu
from jax.sharding import PartitionSpec as P

EPS = 1e-06
LIMIT = 7.0
SIG = 1.702
F32 = jnp.float32
BF16 = jnp.bfloat16
N_REMOTE = 96
N_LOCAL = 48


def iota(shape, dim):
    return lax.broadcasted_iota(jnp.int32, shape, dim)


def sigmoid(x):
    return 1.0 / (1.0 + jnp.exp(-x))


def mm(a, b):
    return jnp.dot(a, b, preferred_element_type=F32)


def body(
    tok_h, mixg_h, wq_h, wk_h, wv_h, wo_h, ig_h, fg_h, mem_h, stab_h, hg_h, dw_h,
    mg_h, eg_h, rt_h, rw_h, w1_h, w3_h, w2_h, og_h,
    out,
    tok, mixg, wa, wb, ig, fg, mem, stab, hg, dt, mg, eg, gains, rt, rw, w1, w3, w2, og,
    nrm, na, xa, xb, sa, sb, ra, rb, sa2, sb2, ra2, rb2, qpad, qt, read,
    mx, gfull, resid, xst, oh_s, ohw_hi, ohw_lo, perm, permt,
    do, di, yst, act, sx, rx, own_x, rst, zo, zi, sq,
    ss, rs, ls, a2a_s, a2a_r,
):
    ep = lax.axis_index("ep")
    t = lax.axis_index("tp")
    z = ep // 8
    y = (ep // 2) % 4
    c = ep % 2
    partner = {"ep": z * 8 + y * 2 + (1 - c)}

    def zdev(zz):
        return {"ep": zz * 8 + y * 2 + c}

    def ydev(yy):
        return {"ep": z * 8 + yy * 2 + c}

    def xdev(xx):
        return {"tp": xx}

    count = [0, 0]
    sent = []

    def rcopy(src, dst, dev):
        i = count[0]
        count[0] += 1
        cp = pltpu.make_async_remote_copy(
            src_ref=src, dst_ref=dst, send_sem=ss.at[i], recv_sem=rs.at[i],
            device_id=dev, device_id_type=pl.DeviceIdType.MESH,
        )
        cp.start()
        sent.append(cp)
        return cp

    def lcopy(src, dst):
        i = count[1]
        count[1] += 1
        cp = pltpu.make_async_copy(src, dst, ls.at[i])
        cp.start()
        return cp

    l_tok = lcopy(tok_h, tok)
    l_mixg = lcopy(mixg_h, mixg)
    l_w = [
        lcopy(wq_h, wa.at[0, z, c]), lcopy(wv_h, wa.at[1, z, c]),
        lcopy(wk_h, wb.at[0, y, c]), lcopy(wo_h, wb.at[1, y, c]),
    ]
    l_g = [lcopy(mg_h, mg), lcopy(eg_h, eg)]
    l_small = [
        lcopy(ig_h, ig), lcopy(fg_h, fg), lcopy(stab_h, stab), lcopy(hg_h, hg),
        lcopy(rt_h, rt), lcopy(rw_h, rw), lcopy(og_h, og),
    ]
    own_rows = pl.ds(pl.multiple_of(t * 512, 512), 512)
    l_dw = lcopy(dw_h.at[:, own_rows], dt.at[z, y, c])

    bar = pltpu.get_barrier_semaphore()
    near = [partner]
    for d in (1, 2, 3):
        near += [zdev((z + d) % 4), ydev((y + d) % 4), xdev((t + d) % 4)]
    for dev in near:
        pl.semaphore_signal(bar, inc=1, device_id=dev, device_id_type=pl.DeviceIdType.MESH)
    pl.semaphore_wait(bar, len(near))

    a_in, b_in = {}, {}
    for d in (2, 1, 3):
        zz, yy = (z + d) % 4, (y + d) % 4
        a_in[d] = [
            rcopy(wq_h, wa.at[0, z, c], zdev(zz)), rcopy(wv_h, wa.at[1, z, c], zdev(zz)),
        ]
        b_in[d] = [
            rcopy(wk_h, wb.at[0, y, c], ydev(yy)), rcopy(wo_h, wb.at[1, y, c], ydev(yy)),
        ]
    p_in = [
        rcopy(wq_h, wa.at[0, z, c], partner), rcopy(wv_h, wa.at[1, z, c], partner),
        rcopy(wk_h, wb.at[0, y, c], partner), rcopy(wo_h, wb.at[1, y, c], partner),
    ]
    l_mem = [lcopy(mem_h.at[pl.ds(2 * i, 2), 0], mem.at[pl.ds(2 * i, 2)]) for i in range(8)]
    l_exp = [lcopy(w1_h.at[0], w1), lcopy(w3_h.at[0], w3), lcopy(w2_h.at[0], w2)]

    l_tok.wait()
    l_mixg.wait()
    x = tok[...].astype(F32)
    ms = jnp.mean(x * x, axis=-1, keepdims=True)
    normed = (x * lax.rsqrt(ms + EPS) * mixg[...]).astype(BF16)
    nrm[...] = normed
    for yy in range(4):
        for zz in range(4):
            na[yy, :, zz * 128:(zz + 1) * 128] = normed[:, zz * 512 + yy * 128:zz * 512 + yy * 128 + 128]
    xa[y] = na[y]
    xb[z] = nrm[:, pl.ds(pl.multiple_of(z * 512, 512), 512)]
    ta_in, tb_in = [], []
    for d in (2, 1, 3):
        zz, yy = (z + d) % 4, (y + d) % 4
        ta_in.append(rcopy(na.at[yy], xa.at[y], ydev(yy)))
        tb_in.append(rcopy(nrm.at[:, pl.ds(pl.multiple_of(zz * 512, 512), 512)], xb.at[z], zdev(zz)))

    da_in, db_in = [], []
    for d in (2, 1, 3):
        zz, yy = (z + d) % 4, (y + d) % 4
        lo = pl.ds(pl.multiple_of(t * 512, 256), 256)
        hi = pl.ds(pl.multiple_of(t * 512 + 256, 256), 256)
        da_in.append(rcopy(dw_h.at[:, lo], dt.at[z, y, c, :, 0:256], zdev(zz)))
        db_in.append(rcopy(dw_h.at[:, hi], dt.at[z, y, c, :, 256:512], ydev(yy)))

    for cp in l_g:
        cp.wait()
    spread = ((iota((64, 128), 1) & 63) == iota((64, 128), 0)).astype(F32)
    mg128 = jnp.dot(jnp.broadcast_to(mg[...], (8, 64)), spread, precision=lax.Precision.HIGHEST, preferred_element_type=F32)
    eg128 = jnp.dot(jnp.broadcast_to(eg[...], (8, 64)), spread, precision=lax.Precision.HIGHEST, preferred_element_type=F32)
    gains[z, y, c] = jnp.where(iota((8, 128), 0) == 0, mg128, eg128)
    g1_in = [rcopy(gains.at[z, y, c], gains.at[z, y, c], zdev((z + d) % 4)) for d in (2, 1, 3)]

    for cp in l_small:
        cp.wait()
    nf = normed.astype(F32)
    log_in = jnp.sum(nf * ig[...].astype(F32), axis=-1, keepdims=True)
    pre_f = jnp.sum(nf * fg[...].astype(F32), axis=-1, keepdims=True)
    log_f = jnp.minimum(pre_f, 0.0) - jnp.log(1.0 + jnp.exp(-jnp.abs(pre_f)))
    eye = iota((16, 16), 0) == iota((16, 16), 1)
    st = jnp.sum(jnp.where(eye, jnp.broadcast_to(stab[...], (16, 16)), 0.0), axis=-1, keepdims=True)
    peak = jnp.maximum(log_f + st, log_in)
    within = jnp.exp(log_in - peak)
    carried = jnp.exp(log_f + st - peak)

    sel = (iota((64, 512), 1) == ep * 16 + (iota((64, 512), 0) & 15))
    col = iota((64, 512), 1)
    cx = jnp.zeros((64, 512), F32)
    wx = jnp.zeros((64, 512), F32)
    for k in range(4):
        r_k = jnp.sum(jnp.where(sel, rt[k:k + 1, :], 0), axis=-1, keepdims=True)
        w_k = jnp.sum(jnp.where(sel, rw[k:k + 1, :], 0.0), axis=-1, keepdims=True)
        hit = ((col >> 4) == r_k).astype(F32)
        cx = cx + hit
        wx = wx + hit * w_k
    r64, c64 = iota((64, 64), 0), iota((64, 64), 1)
    lower = (((r64 >> 4) == (c64 >> 4)) & (c64 < r64)).astype(BF16)
    before = mm(lower, cx.astype(BF16))
    fits = (before == (col & 3).astype(F32)) & (((col >> 2) & 3) == (iota((64, 512), 0) >> 4))
    oh = jnp.where(fits, cx, 0.0)
    oh_s[...] = jnp.transpose(oh).astype(BF16)
    ohw = oh * wx
    hi_part = ohw.astype(BF16)
    ohw_hi[...] = hi_part
    ohw_lo[...] = (ohw - hi_part.astype(F32)).astype(BF16)
    r5, c5 = iota((512, 512), 0), iota((512, 512), 1)
    perm[...] = (c5 == 16 * ((r5 & 127) >> 2) + 4 * (r5 >> 7) + (r5 & 3)).astype(BF16)
    permt[...] = (r5 == 16 * ((c5 & 127) >> 2) + 4 * (c5 >> 7) + (c5 & 3)).astype(BF16)

    f_in = []
    for n, d in enumerate((1, 3, 2)):
        zz, yy = (z + 4 - d) % 4, (y + 4 - d) % 4
        for cp in a_in[d]:
            cp.wait_recv()
        f_in.append(rcopy(wa.at[:, zz, c], wa.at[:, zz, c], partner))
        for cp in b_in[d]:
            cp.wait_recv()
        f_in.append(rcopy(wb.at[:, yy, c], wb.at[:, yy, c], partner))
    for cp in ta_in + tb_in:
        cp.wait_recv()
    for cp in l_w:
        cp.wait()
    for cp in p_in + f_in:
        cp.wait_recv()

    ax = xa[...].reshape(64, 512)
    bx = xb[...].reshape(64, 512)
    sa[...] = mm(ax, wa[0].reshape(512, 512)).reshape(4, 16, 512)
    sb[...] = mm(bx, wb[0].reshape(512, 512)).reshape(4, 16, 512)
    pr_in = []
    for d in (2, 1, 3):
        zz, yy = (z + d) % 4, (y + d) % 4
        pr_in.append(rcopy(sa.at[yy], ra.at[y], ydev(yy)))
        pr_in.append(rcopy(sb.at[zz], rb.at[z], zdev(zz)))
    sa2[...] = mm(ax, wa[1].reshape(512, 512)).astype(BF16).reshape(4, 16, 512)
    sb2[...] = mm(bx, wb[1].reshape(512, 512)).astype(BF16).reshape(4, 16, 512)
    for d in (2, 1, 3):
        zz, yy = (z + d) % 4, (y + d) % 4
        pr_in.append(rcopy(sa2.at[yy], ra2.at[y], ydev(yy)))
        pr_in.append(rcopy(sb2.at[zz], rb2.at[z], zdev(zz)))
    ra[y] = sa[y]
    rb[z] = sb[z]
    ra2[y] = sa2[y]
    rb2[z] = sb2[z]

    l_dw.wait()
    for cp in da_in + db_in + g1_in:
        cp.wait_recv()
    d2_in = []
    for d in (2, 1, 3):
        zz, yy = (z + d) % 4, (y + d) % 4
        d2_in.append(rcopy(gains.at[:, y, c], gains.at[:, y, c], ydev(yy)))
        d2_in.append(rcopy(dt.at[:, y, c, :, 0:256], dt.at[:, y, c, :, 0:256], ydev(yy)))
        d2_in.append(rcopy(dt.at[z, :, c, :, 256:512], dt.at[z, :, c, :, 256:512], zdev(zz)))

    for cp in pr_in:
        cp.wait_recv()
    q = jnp.sum(ra[...], axis=0).astype(BF16).astype(F32) * (512.0 ** -0.5)
    key = jnp.sum(rb[...], axis=0).astype(BF16).astype(F32)
    val = jnp.sum(ra2[...].astype(F32), axis=0)
    og_pre = jnp.sum(rb2[...].astype(F32), axis=0)
    qpad[0:16, :] = q
    qpad[16:128, :] = jnp.zeros((112, 512), F32)
    qt[...] = jnp.transpose(qpad[...])
    for cp in l_mem:
        cp.wait()
    for n in range(16):
        qcol = qt[:, n:n + 1]
        read[n:n + 1, :] = jnp.sum(qcol * mem[n], axis=0, keepdims=True)

    for cp in d2_in:
        cp.wait_recv()
    d3_in = [
        rcopy(dt.at[:, :, c], dt.at[:, :, c], partner),
        rcopy(gains.at[:, :, c], gains.at[:, :, c], partner),
    ]
    score = jnp.sum(q * key, axis=-1, keepdims=True) * within
    rd = score * val + carried * read[...]
    mean = jnp.mean(rd, axis=-1, keepdims=True)
    cen = rd - mean
    var = jnp.mean(cen * cen, axis=-1, keepdims=True)
    gated = (cen * lax.rsqrt(var + EPS) * hg[...] * sigmoid(og_pre)).astype(BF16)
    for cp in d3_in:
        cp.wait_recv()

    part = lax.dot_general(
        gated, dt[...].reshape(2048, 512), (((1,), (1,)), ((), ())), preferred_element_type=F32
    )
    mx[t] = part.astype(BF16)
    m_in = [rcopy(mx.at[t], mx.at[t], xdev((t + d) % 4)) for d in (2, 1, 3)]
    low = iota((1, 128), 1) < 64
    for zz in range(4):
        for yy in range(4):
            at = zz * 512 + yy * 128
            g0, g1 = gains[zz, yy, 0], gains[zz, yy, 1]
            gfull[:, at:at + 128] = jnp.where(low, g0, g1)
    for cp in m_in:
        cp.wait_recv()
    mixed = jnp.sum(mx[...].astype(F32), axis=0)
    xf = tok[...].astype(F32)
    mixed_gain = gfull[0:1, :]
    expert_gain = gfull[1:2, :]
    rf = xf + mixed * lax.rsqrt(jnp.mean(mixed * mixed, axis=-1, keepdims=True) + EPS) * mixed_gain
    resid[...] = rf.astype(BF16)
    ein = (rf * lax.rsqrt(jnp.mean(rf * rf, axis=-1, keepdims=True) + EPS) * expert_gain).astype(BF16)
    for k in range(4):
        xst[k * 16:(k + 1) * 16, :] = ein[:, k * 512:(k + 1) * 512]

    do[...] = mm(oh_s[...], xst[...]).astype(BF16)

    def peer_of(i):
        zz = (z + i // 8 + 2) % 4
        yy = (y + (i // 2) % 4 + 2) % 4
        cc = (c + i % 2) % 2
        return zz * 8 + yy * 2 + cc

    me16 = pl.ds(pl.multiple_of(ep * 16, 16), 16)

    def exchange(src, dst, k):
        def one(i, _):
            p = peer_of(i)
            rows = pl.ds(pl.multiple_of(p * 16, 16), 16)

            @pl.when(p != ep)
            def _():
                pltpu.make_async_remote_copy(
                    src_ref=src.at[rows, :], dst_ref=dst.at[me16, :],
                    send_sem=a2a_s.at[k], recv_sem=a2a_r.at[k],
                    device_id={"ep": p}, device_id_type=pl.DeviceIdType.MESH,
                ).start()
            return 0

        lax.fori_loop(0, 32, one, 0)
        dst[me16, :] = src[me16, :]
        return pltpu.make_async_remote_copy(
            src_ref=src.at[0:496, :], dst_ref=dst.at[0:496, :],
            send_sem=a2a_s.at[k], recv_sem=a2a_r.at[k],
            device_id=partner, device_id_type=pl.DeviceIdType.MESH,
        )

    ex1 = exchange(do, di, 0)
    for cp in l_exp:
        cp.wait()
    ex1.wait_recv()
    yst[...] = mm(perm[...], di[...]).astype(BF16)
    gate = jnp.zeros((128, 512), F32)
    up = jnp.zeros((128, 512), F32)
    for k in range(4):
        rows = yst[k * 128:(k + 1) * 128, :]
        gate = gate + mm(rows, w1[k * 512:(k + 1) * 512, :])
        up = up + mm(rows, w3[k * 512:(k + 1) * 512, :])
    gate = jnp.minimum(gate, LIMIT)
    up = jnp.clip(up, -LIMIT, LIMIT)
    act[...] = ((up + 1.0) * gate * sigmoid(SIG * gate)).astype(BF16)
    x_in = []
    for d in (2, 1, 3):
        tt = (t + d) % 4
        blk = mm(act[...], w2[:, pl.ds(pl.multiple_of(tt * 512, 512), 512)])
        sx[d - 1] = blk.astype(BF16)
        x_in.append(rcopy(sx.at[d - 1], rx.at[d - 1], xdev(tt)))
    own_x[...] = mm(act[...], w2[:, own_rows])
    for cp in x_in:
        cp.wait_recv()
    red = own_x[...] + jnp.sum(rx[...].astype(F32), axis=0)
    redb = red.astype(BF16)
    for k in range(4):
        rst[k * 128:(k + 1) * 128, :] = redb[:, k * 128:(k + 1) * 128]
    zo[...] = mm(permt[...], rst[...]).astype(BF16)
    ex2 = exchange(zo, zi, 1)
    ex2.wait_recv()
    comb4 = mm(ohw_hi[...], zi[...]) + mm(ohw_lo[...], zi[...])
    comb = jnp.concatenate([comb4[k * 16:(k + 1) * 16, :] for k in range(4)], axis=1)
    sq[t] = jnp.broadcast_to(jnp.sum(comb * comb, axis=-1, keepdims=True), (16, 128))
    s_in = [rcopy(sq.at[t], sq.at[t], xdev((t + d) % 4)) for d in (2, 1, 3)]
    for cp in s_in:
        cp.wait_recv()
    total = jnp.sum(sq[...], axis=0)[:, 0:1]
    mine = resid[:, own_rows].astype(F32)
    out[...] = (mine + comb * lax.rsqrt(total * (1.0 / 2048.0) + EPS) * og[...]).astype(BF16)
    for cp in sent:
        cp.wait_send()
    ex1.wait_send()
    ex2.wait_send()


def shards(
    tokens, mixer_gain, query_weight, key_weight, value_weight, outgate_weight,
    igate_weight, fgate_weight, memory, stabilizer, head_gain, down_weight,
    mixed_gain, expert_gain, routes, route_weights, gate_proj, up_proj, expert_down, output_gain,
):
    V = pltpu.VMEM
    scratch = [
        V((16, 2048), BF16), V((1, 2048), F32),
        V((2, 4, 2, 64, 512), BF16), V((2, 4, 2, 64, 512), BF16),
        V((1, 2048), BF16), V((1, 2048), BF16),
        V((16, 512, 512), F32), V((1, 16), F32), V((1, 512), F32),
        V((4, 4, 2, 64, 512), BF16),
        V((1, 64), F32), V((1, 64), F32), V((4, 4, 2, 8, 128), F32),
        V((4, 512), jnp.int32), V((4, 512), F32),
        V((2048, 512), BF16), V((2048, 512), BF16), V((512, 2048), BF16), V((1, 512), F32),
        V((16, 2048), BF16), V((4, 16, 512), BF16), V((4, 16, 512), BF16), V((4, 16, 512), BF16),
        V((4, 16, 512), F32), V((4, 16, 512), F32), V((4, 16, 512), F32), V((4, 16, 512), F32),
        V((4, 16, 512), BF16), V((4, 16, 512), BF16), V((4, 16, 512), BF16), V((4, 16, 512), BF16),
        V((128, 512), F32), V((512, 128), F32), V((16, 512), F32),
        V((4, 16, 2048), BF16), V((8, 2048), F32), V((16, 2048), BF16), V((64, 512), BF16),
        V((512, 64), BF16), V((64, 512), BF16), V((64, 512), BF16),
        V((512, 512), BF16), V((512, 512), BF16),
        V((512, 512), BF16), V((512, 512), BF16), V((512, 512), BF16), V((128, 512), BF16),
        V((3, 128, 512), BF16), V((3, 128, 512), BF16), V((128, 512), F32), V((512, 128), BF16),
        V((512, 128), BF16), V((512, 128), BF16), V((4, 16, 128), F32),
        pltpu.SemaphoreType.DMA((N_REMOTE,)), pltpu.SemaphoreType.DMA((N_REMOTE,)),
        pltpu.SemaphoreType.DMA((N_LOCAL,)),
        pltpu.SemaphoreType.DMA((2,)), pltpu.SemaphoreType.DMA((2,)),
    ]
    return pl.pallas_call(
        body,
        out_shape=jax.ShapeDtypeStruct((16, 512), BF16),
        in_specs=[pl.BlockSpec(memory_space=pl.ANY)] * 20,
        out_specs=pl.BlockSpec(memory_space=pltpu.VMEM),
        scratch_shapes=scratch,
        compiler_params=pltpu.CompilerParams(
            collective_id=0, has_side_effects=True, vmem_limit_bytes=56 * 1024 * 1024
        ),
        name="step",
    )(
        tokens, mixer_gain.reshape(1, 2048), query_weight, key_weight, value_weight, outgate_weight,
        igate_weight, fgate_weight, memory, stabilizer.T, head_gain.reshape(1, 512), down_weight.T,
        mixed_gain.reshape(1, 64), expert_gain.reshape(1, 64), routes.T, route_weights.T,
        gate_proj, up_proj, expert_down, output_gain.reshape(1, 512),
    )


def solution(mesh):
    placed = (
        P("ep", None), P(), P("ep", "tp"), P("ep", "tp"), P("ep", "tp"), P("ep", "tp"),
        P("tp", None), P("tp", None), P("ep", "tp", None, None), P("ep", "tp"), P("tp"),
        P(None, "ep"), P("ep"), P("ep"), P(), P(), P("ep", None, "tp"), P("ep", None, "tp"),
        P("ep", "tp", None), P("tp"),
    )
    return jax.shard_map(
        shards, mesh=mesh, in_specs=placed, out_specs=P("ep", "tp"), check_vma=False
    )
```

```python
import functools
import jax
import jax.numpy as jnp
from jax import lax
from jax.experimental import pallas as pl
from jax.experimental.pallas import tpu as pltpu
from jax.sharding import PartitionSpec as P

EPS = 1e-06
LIMIT = 7.0
SIG = 1.702
F32 = jnp.float32
BF16 = jnp.bfloat16
N_SEND = 14
N_RECV = 19
N_LOCAL = 15


def iota(shape, dim):
    return lax.broadcasted_iota(jnp.int32, shape, dim)


def sigmoid(x):
    return 1.0 / (1.0 + jnp.exp(-x))


def mm(a, b):
    return jnp.dot(a, b, preferred_element_type=F32)


def body(
    tok_h, mixg_h, wq_h, wk_h, wv_h, wo_h, ig_h, fg_h, mem_h, stab_h, hg_h, dw_h,
    mg_h, eg_h, rt_h, rw_h, w1_h, w3_h, w2_h, og_h,
    out,
    tok, mixg, wa, wb, ig, fg, mem, stab, hg, dt, mg, eg, gains, rt, rw, w1, w3, w2, og,
    nrm, na, xa, xb, sa, sb, ra, rb, sa2, sb2, ra2, rb2, qpad, qt, read,
    mx, gfull, resid, xst, oh_s, ohw_hi, ohw_lo, perm, permt,
    do, di, yst, act, sx, rx, own_x, rst, zo, zi, sq,
    ss, rs, ls, a2a_s, a2a_r,
):
    ep = lax.axis_index("ep")
    t = lax.axis_index("tp")
    z = ep // 8
    y = (ep // 2) % 4
    c = ep % 2
    partner = {"ep": z * 8 + y * 2 + (1 - c)}

    def zdev(zz):
        return {"ep": zz * 8 + y * 2 + c}

    def ydev(yy):
        return {"ep": z * 8 + yy * 2 + c}

    def xdev(xx):
        return {"tp": xx}

    sems = [0, 0, 0]

    def ssem():
        sems[0] += 1
        return ss.at[sems[0] - 1]

    def rsem():
        sems[1] += 1
        return rs.at[sems[1] - 1]

    def lsem():
        sems[2] += 1
        return ls.at[sems[2] - 1]

    def rcopy(src, dst, dev, s_sem, r_sem, go=True):
        cp = pltpu.make_async_remote_copy(
            src_ref=src, dst_ref=dst, send_sem=s_sem, recv_sem=r_sem,
            device_id=dev, device_id_type=pl.DeviceIdType.MESH,
        )
        if go:
            cp.start()
        return cp

    ends = []

    def group(like):
        s_sem, r_sem = ssem(), rsem()
        whole = rcopy(like, like, partner, s_sem, r_sem, go=False)
        ends.append(whole)
        return s_sem, r_sem, whole

    def lcopy(src, dst, sem=None):
        cp = pltpu.make_async_copy(src, dst, lsem() if sem is None else sem)
        cp.start()
        return cp

    w_sem = lsem()
    l_w = [
        lcopy(wq_h, wa.at[0, z, c], w_sem), lcopy(wv_h, wa.at[1, z, c], w_sem),
        lcopy(wk_h, wb.at[0, y, c], w_sem), lcopy(wo_h, wb.at[1, y, c], w_sem),
    ]
    own_rows = pl.ds(pl.multiple_of(t * 512, 512), 512)
    l_dw = lcopy(dw_h.at[:, own_rows], dt.at[z, y, c])
    l_g = [lcopy(mg_h, mg), lcopy(eg_h, eg)]
    l_tok = lcopy(tok_h, tok)
    l_mixg = lcopy(mixg_h, mixg)
    l_small = [
        lcopy(ig_h, ig), lcopy(fg_h, fg), lcopy(stab_h, stab), lcopy(hg_h, hg),
        lcopy(rt_h, rt), lcopy(rw_h, rw), lcopy(og_h, og),
    ]

    bar = pltpu.get_barrier_semaphore()
    near = [partner]
    for d in (1, 2, 3):
        near += [zdev((z + d) % 4), ydev((y + d) % 4), xdev((t + d) % 4)]
    for dev in near:
        pl.semaphore_signal(bar, inc=1, device_id=dev, device_id_type=pl.DeviceIdType.MESH)

    for cp in l_g:
        cp.wait()
    spread = ((iota((64, 128), 1) & 63) == iota((64, 128), 0)).astype(F32)
    mg128 = jnp.dot(jnp.broadcast_to(mg[...], (8, 64)), spread, precision=lax.Precision.HIGHEST, preferred_element_type=F32)
    eg128 = jnp.dot(jnp.broadcast_to(eg[...], (8, 64)), spread, precision=lax.Precision.HIGHEST, preferred_element_type=F32)
    gains[z, y, c] = jnp.where(iota((8, 128), 0) == 0, mg128, eg128)
    l_dw.wait()
    pltpu.make_async_copy(wa.at[:, 0:1], wa.at[:, 0:1], w_sem).wait()
    pl.semaphore_wait(bar, len(near))

    s1, r1, d1_in = group(dt.at[0:3, 0, 0])
    g1s, g1r, g1_in = group(gains.at[0:3, 0, 0])
    for d in (2, 1, 3):
        zz, yy = (z + d) % 4, (y + d) % 4
        rcopy(dt.at[z, y, c, :, 0:256], dt.at[z, y, c, :, 0:256], zdev(zz), s1, r1)
        rcopy(dt.at[z, y, c, :, 256:512], dt.at[z, y, c, :, 256:512], ydev(yy), s1, r1)
        rcopy(gains.at[z, y, c], gains.at[z, y, c], zdev(zz), g1s, g1r)

    sw, rp, p_in = group(wa)
    a_in, b_in = {}, {}
    for d in (2, 1, 3):
        zz, yy = (z + d) % 4, (y + d) % 4
        a_in[d] = rcopy(wa.at[:, z, c], wa.at[:, z, c], zdev(zz), sw, rsem())
        b_in[d] = rcopy(wb.at[:, y, c], wb.at[:, y, c], ydev(yy), sw, rsem())
    rcopy(wa.at[:, z, c], wa.at[:, z, c], partner, sw, rp)
    rcopy(wb.at[:, y, c], wb.at[:, y, c], partner, sw, rp)
    sf = ssem()
    ends.append(rcopy(wa.at[:, 0:3], wa.at[:, 0:3], partner, sf, rp, go=False))

    l_tok.wait()
    l_mixg.wait()
    x = tok[...].astype(F32)
    ms = jnp.mean(x * x, axis=-1, keepdims=True)
    normed = (x * lax.rsqrt(ms + EPS) * mixg[...]).astype(BF16)
    nrm[...] = normed
    for yy in range(4):
        for zz in range(4):
            na[yy, :, zz * 128:(zz + 1) * 128] = normed[:, zz * 512 + yy * 128:zz * 512 + yy * 128 + 128]
    xa[y] = na[y]
    xb[z] = nrm[:, pl.ds(pl.multiple_of(z * 512, 512), 512)]
    st_, rt_, t_in = group(ra.at[0:3])
    for d in (2, 1, 3):
        zz, yy = (z + d) % 4, (y + d) % 4
        rcopy(na.at[yy], xa.at[y], ydev(yy), st_, rt_)
        rcopy(nrm.at[:, pl.ds(pl.multiple_of(zz * 512, 512), 512)], xb.at[z], zdev(zz), st_, rt_)

    m_sem, e_sem = lsem(), lsem()
    for i in range(8):
        lcopy(mem_h.at[pl.ds(2 * i, 2), 0], mem.at[pl.ds(2 * i, 2)], m_sem)
    for src, dst in ((w1_h, w1), (w3_h, w3), (w2_h, w2)):
        lcopy(src.at[0], dst, e_sem)

    for cp in l_small:
        cp.wait()
    nf = normed.astype(F32)
    log_in = jnp.sum(nf * ig[...].astype(F32), axis=-1, keepdims=True)
    pre_f = jnp.sum(nf * fg[...].astype(F32), axis=-1, keepdims=True)
    log_f = jnp.minimum(pre_f, 0.0) - jnp.log(1.0 + jnp.exp(-jnp.abs(pre_f)))
    eye = iota((16, 16), 0) == iota((16, 16), 1)
    st = jnp.sum(jnp.where(eye, jnp.broadcast_to(stab[...], (16, 16)), 0.0), axis=-1, keepdims=True)
    peak = jnp.maximum(log_f + st, log_in)
    within = jnp.exp(log_in - peak)
    carried = jnp.exp(log_f + st - peak)

    sel = (iota((64, 512), 1) == ep * 16 + (iota((64, 512), 0) & 15))
    col = iota((64, 512), 1)
    cx = jnp.zeros((64, 512), F32)
    wx = jnp.zeros((64, 512), F32)
    for k in range(4):
        r_k = jnp.sum(jnp.where(sel, rt[k:k + 1, :], 0), axis=-1, keepdims=True)
        w_k = jnp.sum(jnp.where(sel, rw[k:k + 1, :], 0.0), axis=-1, keepdims=True)
        hit = ((col >> 4) == r_k).astype(F32)
        cx = cx + hit
        wx = wx + hit * w_k
    r64, c64 = iota((64, 64), 0), iota((64, 64), 1)
    lower = (((r64 >> 4) == (c64 >> 4)) & (c64 < r64)).astype(BF16)
    before = mm(lower, cx.astype(BF16))
    fits = (before == (col & 3).astype(F32)) & (((col >> 2) & 3) == (iota((64, 512), 0) >> 4))
    oh = jnp.where(fits, cx, 0.0)
    oh_s[...] = jnp.transpose(oh).astype(BF16)
    ohw = oh * wx
    hi_part = ohw.astype(BF16)
    ohw_hi[...] = hi_part
    ohw_lo[...] = (ohw - hi_part.astype(F32)).astype(BF16)
    r5, c5 = iota((512, 512), 0), iota((512, 512), 1)
    perm[...] = (c5 == 16 * ((r5 & 127) >> 2) + 4 * (r5 >> 7) + (r5 & 3)).astype(BF16)
    permt[...] = (r5 == 16 * ((c5 & 127) >> 2) + 4 * (c5 >> 7) + (c5 & 3)).astype(BF16)

    d1_in.wait_recv()
    g1_in.wait_recv()
    s2, r2, d2_in = group(dt.at[0:3, :, 0])
    g2s, g2r, g2_in = group(gains.at[0:3, :, 0])
    for d in (2, 1, 3):
        zz, yy = (z + d) % 4, (y + d) % 4
        rcopy(gains.at[:, y, c], gains.at[:, y, c], ydev(yy), g2s, g2r)
        rcopy(dt.at[:, y, c, :, 0:256], dt.at[:, y, c, :, 0:256], ydev(yy), s2, r2)
        rcopy(dt.at[z, :, c, :, 256:512], dt.at[z, :, c, :, 256:512], zdev(zz), s2, r2)

    for d in (1, 3, 2):
        zz, yy = (z + 4 - d) % 4, (y + 4 - d) % 4
        a_in[d].wait_recv()
        rcopy(wa.at[:, zz, c], wa.at[:, zz, c], partner, sf, rp)
        b_in[d].wait_recv()
        rcopy(wb.at[:, yy, c], wb.at[:, yy, c], partner, sf, rp)
    t_in.wait_recv()
    p_in.wait_recv()

    ax = xa[...].reshape(64, 512)
    bx = xb[...].reshape(64, 512)
    sa[...] = mm(ax, wa[0].reshape(512, 512)).reshape(4, 16, 512)
    sb[...] = mm(bx, wb[0].reshape(512, 512)).reshape(4, 16, 512)
    sq_, rq_, q_in = group(dt.at[0:3, 0, 0])
    sv_, rv_, v_in = group(ra.at[0:3])
    for d in (2, 1, 3):
        zz, yy = (z + d) % 4, (y + d) % 4
        rcopy(sa.at[yy], ra.at[y], ydev(yy), sq_, rq_)
        rcopy(sb.at[zz], rb.at[z], zdev(zz), sq_, rq_)
    sa2[...] = mm(ax, wa[1].reshape(512, 512)).astype(BF16).reshape(4, 16, 512)
    sb2[...] = mm(bx, wb[1].reshape(512, 512)).astype(BF16).reshape(4, 16, 512)
    for d in (2, 1, 3):
        zz, yy = (z + d) % 4, (y + d) % 4
        rcopy(sa2.at[yy], ra2.at[y], ydev(yy), sv_, rv_)
        rcopy(sb2.at[zz], rb2.at[z], zdev(zz), sv_, rv_)
    ra[y] = sa[y]
    rb[z] = sb[z]
    ra2[y] = sa2[y]
    rb2[z] = sb2[z]

    d2_in.wait_recv()
    g2_in.wait_recv()
    s3, r3, d3_in = group(dt.at[:, :, 0])
    g3s, g3r, g3_in = group(gains.at[:, :, 0])
    rcopy(dt.at[:, :, c], dt.at[:, :, c], partner, s3, r3)
    rcopy(gains.at[:, :, c], gains.at[:, :, c], partner, g3s, g3r)

    q_in.wait_recv()
    v_in.wait_recv()
    q = jnp.sum(ra[...], axis=0).astype(BF16).astype(F32) * (512.0 ** -0.5)
    key = jnp.sum(rb[...], axis=0).astype(BF16).astype(F32)
    val = jnp.sum(ra2[...].astype(F32), axis=0)
    og_pre = jnp.sum(rb2[...].astype(F32), axis=0)
    qpad[0:16, :] = q
    qpad[16:128, :] = jnp.zeros((112, 512), F32)
    qt[...] = jnp.transpose(qpad[...])
    pltpu.make_async_copy(mem, mem, m_sem).wait()
    for n in range(16):
        qcol = qt[:, n:n + 1]
        read[n:n + 1, :] = jnp.sum(qcol * mem[n], axis=0, keepdims=True)

    score = jnp.sum(q * key, axis=-1, keepdims=True) * within
    rd = score * val + carried * read[...]
    mean = jnp.mean(rd, axis=-1, keepdims=True)
    cen = rd - mean
    var = jnp.mean(cen * cen, axis=-1, keepdims=True)
    gated = (cen * lax.rsqrt(var + EPS) * hg[...] * sigmoid(og_pre)).astype(BF16)
    d3_in.wait_recv()
    g3_in.wait_recv()
    sm, rm, m_in = group(mx.at[0:3])
    for k in range(4):
        cols = pl.ds(k * 512, 512)
        part = lax.dot_general(
            gated, dt[k].reshape(512, 512), (((1,), (1,)), ((), ())), preferred_element_type=F32
        )
        mx[t, :, cols] = part.astype(BF16)
        for d in (2, 1, 3):
            rcopy(mx.at[t, :, cols], mx.at[t, :, cols], xdev((t + d) % 4), sm, rm)
    low = iota((1, 128), 1) < 64
    for zz in range(4):
        for yy in range(4):
            at = zz * 512 + yy * 128
            g0, g1 = gains[zz, yy, 0], gains[zz, yy, 1]
            gfull[:, at:at + 128] = jnp.where(low, g0, g1)
    m_in.wait_recv()
    mixed = jnp.sum(mx[...].astype(F32), axis=0)
    xf = tok[...].astype(F32)
    mixed_gain = gfull[0:1, :]
    expert_gain = gfull[1:2, :]
    rf = xf + mixed * lax.rsqrt(jnp.mean(mixed * mixed, axis=-1, keepdims=True) + EPS) * mixed_gain
    resid[...] = rf.astype(BF16)
    ein = (rf * lax.rsqrt(jnp.mean(rf * rf, axis=-1, keepdims=True) + EPS) * expert_gain).astype(BF16)
    for k in range(4):
        xst[k * 16:(k + 1) * 16, :] = ein[:, k * 512:(k + 1) * 512]

    do[...] = mm(oh_s[...], xst[...]).astype(BF16)

    def peer_of(i):
        zz = (z + i // 8 + 2) % 4
        yy = (y + (i // 2) % 4 + 2) % 4
        cc = (c + i % 2) % 2
        return zz * 8 + yy * 2 + cc

    me16 = pl.ds(pl.multiple_of(ep * 16, 16), 16)

    def exchange(src, dst, k):
        def one(i, _):
            p = peer_of(i)
            rows = pl.ds(pl.multiple_of(p * 16, 16), 16)

            @pl.when(p != ep)
            def _():
                pltpu.make_async_remote_copy(
                    src_ref=src.at[rows, :], dst_ref=dst.at[me16, :],
                    send_sem=a2a_s.at[k], recv_sem=a2a_r.at[k],
                    device_id={"ep": p}, device_id_type=pl.DeviceIdType.MESH,
                ).start()
            return 0

        lax.fori_loop(0, 32, one, 0)
        dst[me16, :] = src[me16, :]
        return pltpu.make_async_remote_copy(
            src_ref=src.at[0:496, :], dst_ref=dst.at[0:496, :],
            send_sem=a2a_s.at[k], recv_sem=a2a_r.at[k],
            device_id=partner, device_id_type=pl.DeviceIdType.MESH,
        )

    ex1 = exchange(do, di, 0)
    pltpu.make_async_copy(mem.at[0:6], mem.at[0:6], e_sem).wait()
    ex1.wait_recv()
    yst[...] = mm(perm[...], di[...]).astype(BF16)
    gate = jnp.zeros((128, 512), F32)
    up = jnp.zeros((128, 512), F32)
    for k in range(4):
        rows = yst[k * 128:(k + 1) * 128, :]
        gate = gate + mm(rows, w1[k * 512:(k + 1) * 512, :])
        up = up + mm(rows, w3[k * 512:(k + 1) * 512, :])
    gate = jnp.minimum(gate, LIMIT)
    up = jnp.clip(up, -LIMIT, LIMIT)
    act[...] = ((up + 1.0) * gate * sigmoid(SIG * gate)).astype(BF16)
    sxs, rxs, x_in = group(rx)
    for d in (2, 1, 3):
        tt = (t + d) % 4
        blk = mm(act[...], w2[:, pl.ds(pl.multiple_of(tt * 512, 512), 512)])
        sx[d - 1] = blk.astype(BF16)
        rcopy(sx.at[d - 1], rx.at[d - 1], xdev(tt), sxs, rxs)
    own_x[...] = mm(act[...], w2[:, own_rows])
    x_in.wait_recv()
    red = own_x[...] + jnp.sum(rx[...].astype(F32), axis=0)
    redb = red.astype(BF16)
    for k in range(4):
        rst[k * 128:(k + 1) * 128, :] = redb[:, k * 128:(k + 1) * 128]
    zo[...] = mm(permt[...], rst[...]).astype(BF16)
    ex2 = exchange(zo, zi, 1)
    ex2.wait_recv()
    comb4 = mm(ohw_hi[...], zi[...]) + mm(ohw_lo[...], zi[...])
    comb = jnp.concatenate([comb4[k * 16:(k + 1) * 16, :] for k in range(4)], axis=1)
    sq[t] = jnp.broadcast_to(jnp.sum(comb * comb, axis=-1, keepdims=True), (16, 128))
    sqs, sqr, s_in = group(sq.at[0:3])
    for d in (2, 1, 3):
        rcopy(sq.at[t], sq.at[t], xdev((t + d) % 4), sqs, sqr)
    s_in.wait_recv()
    total = jnp.sum(sq[...], axis=0)[:, 0:1]
    mine = resid[:, own_rows].astype(F32)
    out[...] = (mine + comb * lax.rsqrt(total * (1.0 / 2048.0) + EPS) * og[...]).astype(BF16)
    for cp in ends:
        cp.wait_send()
    ex1.wait_send()
    ex2.wait_send()
    assert sems == [N_SEND, N_RECV, N_LOCAL], sems


def shards(
    tokens, mixer_gain, query_weight, key_weight, value_weight, outgate_weight,
    igate_weight, fgate_weight, memory, stabilizer, head_gain, down_weight,
    mixed_gain, expert_gain, routes, route_weights, gate_proj, up_proj, expert_down, output_gain,
):
    V = pltpu.VMEM
    scratch = [
        V((16, 2048), BF16), V((1, 2048), F32),
        V((2, 4, 2, 64, 512), BF16), V((2, 4, 2, 64, 512), BF16),
        V((1, 2048), BF16), V((1, 2048), BF16),
        V((16, 512, 512), F32), V((1, 16), F32), V((1, 512), F32),
        V((4, 4, 2, 64, 512), BF16),
        V((1, 64), F32), V((1, 64), F32), V((4, 4, 2, 8, 128), F32),
        V((4, 512), jnp.int32), V((4, 512), F32),
        V((2048, 512), BF16), V((2048, 512), BF16), V((512, 2048), BF16), V((1, 512), F32),
        V((16, 2048), BF16), V((4, 16, 512), BF16), V((4, 16, 512), BF16), V((4, 16, 512), BF16),
        V((4, 16, 512), F32), V((4, 16, 512), F32), V((4, 16, 512), F32), V((4, 16, 512), F32),
        V((4, 16, 512), BF16), V((4, 16, 512), BF16), V((4, 16, 512), BF16), V((4, 16, 512), BF16),
        V((128, 512), F32), V((512, 128), F32), V((16, 512), F32),
        V((4, 16, 2048), BF16), V((8, 2048), F32), V((16, 2048), BF16), V((64, 512), BF16),
        V((512, 64), BF16), V((64, 512), BF16), V((64, 512), BF16),
        V((512, 512), BF16), V((512, 512), BF16),
        V((512, 512), BF16), V((512, 512), BF16), V((512, 512), BF16), V((128, 512), BF16),
        V((3, 128, 512), BF16), V((3, 128, 512), BF16), V((128, 512), F32), V((512, 128), BF16),
        V((512, 128), BF16), V((512, 128), BF16), V((4, 16, 128), F32),
        pltpu.SemaphoreType.DMA((N_SEND,)), pltpu.SemaphoreType.DMA((N_RECV,)),
        pltpu.SemaphoreType.DMA((N_LOCAL,)),
        pltpu.SemaphoreType.DMA((2,)), pltpu.SemaphoreType.DMA((2,)),
    ]
    return pl.pallas_call(
        body,
        out_shape=jax.ShapeDtypeStruct((16, 512), BF16),
        in_specs=[pl.BlockSpec(memory_space=pl.ANY)] * 20,
        out_specs=pl.BlockSpec(memory_space=pltpu.VMEM),
        scratch_shapes=scratch,
        compiler_params=pltpu.CompilerParams(
            collective_id=0, has_side_effects=True, vmem_limit_bytes=56 * 1024 * 1024
        ),
        name="step",
    )(
        tokens, mixer_gain.reshape(1, 2048), query_weight, key_weight, value_weight, outgate_weight,
        igate_weight, fgate_weight, memory, stabilizer.T, head_gain.reshape(1, 512), down_weight.T,
        mixed_gain.reshape(1, 64), expert_gain.reshape(1, 64), routes.T, route_weights.T,
        gate_proj, up_proj, expert_down, output_gain.reshape(1, 512),
    )


def solution(mesh):
    placed = (
        P("ep", None), P(), P("ep", "tp"), P("ep", "tp"), P("ep", "tp"), P("ep", "tp"),
        P("tp", None), P("tp", None), P("ep", "tp", None, None), P("ep", "tp"), P("tp"),
        P(None, "ep"), P("ep"), P("ep"), P(), P(), P("ep", None, "tp"), P("ep", None, "tp"),
        P("ep", "tp", None), P("tp"),
    )
    return jax.shard_map(
        shards, mesh=mesh, in_specs=placed, out_specs=P("ep", "tp"), check_vma=False
    )
```

```python
import functools
import jax
import jax.numpy as jnp
from jax import lax
from jax.experimental import pallas as pl
from jax.experimental.pallas import tpu as pltpu
from jax.sharding import PartitionSpec as P

EPS = 1e-06
LIMIT = 7.0
SIG = 1.702
F32 = jnp.float32
BF16 = jnp.bfloat16
N_SEND = 15
N_RECV = 20
N_LOCAL = 15


def iota(shape, dim):
    return lax.broadcasted_iota(jnp.int32, shape, dim)


def sigmoid(x):
    return 1.0 / (1.0 + jnp.exp(-x))


def mm(a, b):
    return jnp.dot(a, b, preferred_element_type=F32)


def body(
    tok_h, mixg_h, wq_h, wk_h, wv_h, wo_h, ig_h, fg_h, mem_h, stab_h, hg_h, dw_h,
    mg_h, eg_h, rt_h, rw_h, w1_h, w3_h, w2_h, og_h,
    out,
    tok, mixg, wa, wb, ig, fg, mem, stab, hg, dt, mg, eg, gains, rt, rw, w1, w3, w2, og,
    nrm, na, xa, xb, sa, sb, ra, rb, qpad, qt, read,
    mx, gfull, resid, xst, oh_s, ohw_hi, ohw_lo, perm, permt,
    do, di, yst, act, sx, rx, own_x, rst, zo, zi, bst, zbo, zbi, cbs, cbr, sq,
    ss, rs, ls, a2a_s, a2a_r,
):
    ep = lax.axis_index("ep")
    t = lax.axis_index("tp")
    z = ep // 8
    y = (ep // 2) % 4
    c = ep % 2
    partner = {"ep": z * 8 + y * 2 + (1 - c)}

    def zdev(zz):
        return {"ep": zz * 8 + y * 2 + c}

    def ydev(yy):
        return {"ep": z * 8 + yy * 2 + c}

    def xdev(xx):
        return {"tp": xx}

    sems = [0, 0, 0]

    def ssem():
        sems[0] += 1
        return ss.at[sems[0] - 1]

    def rsem():
        sems[1] += 1
        return rs.at[sems[1] - 1]

    def lsem():
        sems[2] += 1
        return ls.at[sems[2] - 1]

    def rcopy(src, dst, dev, s_sem, r_sem, go=True):
        cp = pltpu.make_async_remote_copy(
            src_ref=src, dst_ref=dst, send_sem=s_sem, recv_sem=r_sem,
            device_id=dev, device_id_type=pl.DeviceIdType.MESH,
        )
        if go:
            cp.start()
        return cp

    ends = []

    def group(like):
        s_sem, r_sem = ssem(), rsem()
        whole = rcopy(like, like, partner, s_sem, r_sem, go=False)
        ends.append(whole)
        return s_sem, r_sem, whole

    def lcopy(src, dst, sem=None):
        cp = pltpu.make_async_copy(src, dst, lsem() if sem is None else sem)
        cp.start()
        return cp

    w_sem = lsem()
    l_w = [
        lcopy(wv_h, wa.at[0, z, c], w_sem), lcopy(wo_h, wa.at[1, z, c], w_sem),
        lcopy(wq_h, wb.at[0, y, c], w_sem), lcopy(wk_h, wb.at[1, y, c], w_sem),
    ]
    own_rows = pl.ds(pl.multiple_of(t * 512, 512), 512)
    l_dw = lcopy(dw_h.at[:, own_rows], dt.at[z, y, c])
    l_g = [lcopy(mg_h, mg), lcopy(eg_h, eg)]
    l_tok = lcopy(tok_h, tok)
    l_mixg = lcopy(mixg_h, mixg)
    l_small = [
        lcopy(ig_h, ig), lcopy(fg_h, fg), lcopy(stab_h, stab), lcopy(hg_h, hg),
        lcopy(rt_h, rt), lcopy(rw_h, rw), lcopy(og_h, og),
    ]

    bar = pltpu.get_barrier_semaphore()
    near = [partner]
    for d in (1, 2, 3):
        near += [zdev((z + d) % 4), ydev((y + d) % 4), xdev((t + d) % 4)]
    for dev in near:
        pl.semaphore_signal(bar, inc=1, device_id=dev, device_id_type=pl.DeviceIdType.MESH)

    for cp in l_g:
        cp.wait()
    spread = ((iota((64, 128), 1) & 63) == iota((64, 128), 0)).astype(F32)
    mg128 = jnp.dot(jnp.broadcast_to(mg[...], (8, 64)), spread, precision=lax.Precision.HIGHEST, preferred_element_type=F32)
    eg128 = jnp.dot(jnp.broadcast_to(eg[...], (8, 64)), spread, precision=lax.Precision.HIGHEST, preferred_element_type=F32)
    gains[z, y, c] = jnp.where(iota((8, 128), 0) == 0, mg128, eg128)
    l_dw.wait()
    pltpu.make_async_copy(wa.at[:, 0:1], wa.at[:, 0:1], w_sem).wait()
    pl.semaphore_wait(bar, len(near))

    s1, r1, d1_in = group(dt.at[0:3, 0, 0])
    g1s, g1r, g1_in = group(gains.at[0:3, 0, 0])
    for d in (2, 1, 3):
        zz, yy = (z + d) % 4, (y + d) % 4
        rcopy(dt.at[z, y, c, :, 0:256], dt.at[z, y, c, :, 0:256], zdev(zz), s1, r1)
        rcopy(dt.at[z, y, c, :, 256:512], dt.at[z, y, c, :, 256:512], ydev(yy), s1, r1)
        rcopy(gains.at[z, y, c], gains.at[z, y, c], zdev(zz), g1s, g1r)

    sw, rp, p_in = group(wa)
    a_in, b_in = {}, {}
    for d in (2, 1, 3):
        zz, yy = (z + d) % 4, (y + d) % 4
        a_in[d] = rcopy(wa.at[:, z, c], wa.at[:, z, c], zdev(zz), sw, rsem())
        b_in[d] = rcopy(wb.at[:, y, c], wb.at[:, y, c], ydev(yy), sw, rsem())
    rcopy(wa.at[:, z, c], wa.at[:, z, c], partner, sw, rp)
    rcopy(wb.at[:, y, c], wb.at[:, y, c], partner, sw, rp)
    sf = ssem()
    ends.append(rcopy(wa.at[:, 0:3], wa.at[:, 0:3], partner, sf, rp, go=False))

    l_tok.wait()
    l_mixg.wait()
    x = tok[...].astype(F32)
    ms = jnp.mean(x * x, axis=-1, keepdims=True)
    normed = (x * lax.rsqrt(ms + EPS) * mixg[...]).astype(BF16)
    nrm[...] = normed
    for yy in range(4):
        for zz in range(4):
            na[yy, :, zz * 128:(zz + 1) * 128] = normed[:, zz * 512 + yy * 128:zz * 512 + yy * 128 + 128]
    xa[y] = na[y]
    xb[z] = nrm[:, pl.ds(pl.multiple_of(z * 512, 512), 512)]
    st_, rt_, t_in = group(ra.at[0:3])
    for d in (2, 1, 3):
        zz, yy = (z + d) % 4, (y + d) % 4
        rcopy(na.at[yy], xa.at[y], ydev(yy), st_, rt_)
        rcopy(nrm.at[:, pl.ds(pl.multiple_of(zz * 512, 512), 512)], xb.at[z], zdev(zz), st_, rt_)

    m_sem, e_sem = lsem(), lsem()
    for i in range(8):
        lcopy(mem_h.at[pl.ds(2 * i, 2), 0], mem.at[pl.ds(2 * i, 2)], m_sem)
    for src, dst in ((w1_h, w1), (w3_h, w3), (w2_h, w2)):
        lcopy(src.at[0], dst, e_sem)

    for cp in l_small:
        cp.wait()
    nf = normed.astype(F32)
    log_in = jnp.sum(nf * ig[...].astype(F32), axis=-1, keepdims=True)
    pre_f = jnp.sum(nf * fg[...].astype(F32), axis=-1, keepdims=True)
    log_f = jnp.minimum(pre_f, 0.0) - jnp.log(1.0 + jnp.exp(-jnp.abs(pre_f)))
    eye = iota((16, 16), 0) == iota((16, 16), 1)
    st = jnp.sum(jnp.where(eye, jnp.broadcast_to(stab[...], (16, 16)), 0.0), axis=-1, keepdims=True)
    peak = jnp.maximum(log_f + st, log_in)
    within = jnp.exp(log_in - peak)
    carried = jnp.exp(log_f + st - peak)

    sel = (iota((64, 512), 1) == ep * 16 + (iota((64, 512), 0) & 15))
    col = iota((64, 512), 1)
    cx = jnp.zeros((64, 512), F32)
    wx = jnp.zeros((64, 512), F32)
    for k in range(4):
        r_k = jnp.sum(jnp.where(sel, rt[k:k + 1, :], 0), axis=-1, keepdims=True)
        w_k = jnp.sum(jnp.where(sel, rw[k:k + 1, :], 0.0), axis=-1, keepdims=True)
        hit = ((col >> 4) == r_k).astype(F32)
        cx = cx + hit
        wx = wx + hit * w_k
    r64, c64 = iota((64, 64), 0), iota((64, 64), 1)
    lower = (((r64 >> 4) == (c64 >> 4)) & (c64 < r64)).astype(BF16)
    before = mm(lower, cx.astype(BF16))
    fits = (before == (col & 3).astype(F32)) & (((col >> 2) & 3) == (iota((64, 512), 0) >> 4))
    oh = jnp.where(fits, cx, 0.0)
    oh_s[...] = jnp.transpose(oh).astype(BF16)
    ohw = oh * wx
    hi_part = ohw.astype(BF16)
    ohw_hi[...] = hi_part
    ohw_lo[...] = (ohw - hi_part.astype(F32)).astype(BF16)
    r5, c5 = iota((512, 512), 0), iota((512, 512), 1)
    perm[...] = (c5 == 16 * ((r5 & 127) >> 2) + 4 * (r5 >> 7) + (r5 & 3)).astype(BF16)
    permt[...] = (r5 == 16 * ((c5 & 127) >> 2) + 4 * (c5 >> 7) + (c5 & 3)).astype(BF16)

    d1_in.wait_recv()
    g1_in.wait_recv()
    s2, r2, d2_in = group(dt.at[0:3, :, 0])
    g2s, g2r, g2_in = group(gains.at[0:3, :, 0])
    for d in (2, 1, 3):
        zz, yy = (z + d) % 4, (y + d) % 4
        rcopy(gains.at[:, y, c], gains.at[:, y, c], ydev(yy), g2s, g2r)
        rcopy(dt.at[:, y, c, :, 0:256], dt.at[:, y, c, :, 0:256], ydev(yy), s2, r2)
        rcopy(dt.at[z, :, c, :, 256:512], dt.at[z, :, c, :, 256:512], zdev(zz), s2, r2)

    for d in (1, 3, 2):
        zz, yy = (z + 4 - d) % 4, (y + 4 - d) % 4
        a_in[d].wait_recv()
        rcopy(wa.at[:, zz, c], wa.at[:, zz, c], partner, sf, rp)
        b_in[d].wait_recv()
        rcopy(wb.at[:, yy, c], wb.at[:, yy, c], partner, sf, rp)
    t_in.wait_recv()
    p_in.wait_recv()

    ax = xa[...].reshape(64, 512)
    bx = xb[...].reshape(64, 512)
    sq_, rq_, q_in = group(dt.at[0:3, 0, 0])
    sv_, rv_, v_in = group(ra.at[0:3])
    for k in range(2):
        cols = pl.ds(k * 512, 512)
        sb[:, :, cols] = mm(bx, wb[k].reshape(512, 512)).reshape(4, 16, 512)
        for d in (2, 1, 3):
            zz = (z + d) % 4
            rcopy(sb.at[zz, :, cols], rb.at[z, :, cols], zdev(zz), sq_, rq_)
    for k in range(2):
        cols = pl.ds(k * 512, 512)
        sa[:, :, cols] = mm(ax, wa[k].reshape(512, 512)).astype(BF16).reshape(4, 16, 512)
        for d in (2, 1, 3):
            yy = (y + d) % 4
            rcopy(sa.at[yy, :, cols], ra.at[y, :, cols], ydev(yy), sv_, rv_)
    ra[y] = sa[y]
    rb[z] = sb[z]

    d2_in.wait_recv()
    g2_in.wait_recv()
    s3, r3, d3_in = group(dt.at[:, :, 0])
    g3s, g3r, g3_in = group(gains.at[:, :, 0])
    rcopy(dt.at[:, :, c], dt.at[:, :, c], partner, s3, r3)
    rcopy(gains.at[:, :, c], gains.at[:, :, c], partner, g3s, g3r)

    q_in.wait_recv()
    v_in.wait_recv()
    qk = jnp.sum(rb[...], axis=0).astype(BF16).astype(F32)
    q = qk[:, 0:512] * (512.0 ** -0.5)
    key = qk[:, 512:]
    vo = jnp.sum(ra[...].astype(F32), axis=0)
    val = vo[:, 0:512]
    og_pre = vo[:, 512:]
    qpad[0:16, :] = q
    qpad[16:128, :] = jnp.zeros((112, 512), F32)
    qt[...] = jnp.transpose(qpad[...])
    pltpu.make_async_copy(mem, mem, m_sem).wait()
    for n in range(16):
        qcol = qt[:, n:n + 1]
        read[n:n + 1, :] = jnp.sum(qcol * mem[n], axis=0, keepdims=True)

    score = jnp.sum(q * key, axis=-1, keepdims=True) * within
    rd = score * val + carried * read[...]
    mean = jnp.mean(rd, axis=-1, keepdims=True)
    cen = rd - mean
    var = jnp.mean(cen * cen, axis=-1, keepdims=True)
    gated = (cen * lax.rsqrt(var + EPS) * hg[...] * sigmoid(og_pre)).astype(BF16)
    d3_in.wait_recv()
    g3_in.wait_recv()
    sm, rm, m_in = group(mx.at[0:3])
    for k in range(4):
        cols = pl.ds(k * 512, 512)
        part = lax.dot_general(
            gated, dt[k].reshape(512, 512), (((1,), (1,)), ((), ())), preferred_element_type=F32
        )
        mx[t, :, cols] = part.astype(BF16)
        for d in (2, 1, 3):
            rcopy(mx.at[t, :, cols], mx.at[t, :, cols], xdev((t + d) % 4), sm, rm)
    low = iota((1, 128), 1) < 64
    for zz in range(4):
        for yy in range(4):
            at = zz * 512 + yy * 128
            g0, g1 = gains[zz, yy, 0], gains[zz, yy, 1]
            gfull[:, at:at + 128] = jnp.where(low, g0, g1)
    m_in.wait_recv()
    mixed = jnp.sum(mx[...].astype(F32), axis=0)
    xf = tok[...].astype(F32)
    mixed_gain = gfull[0:1, :]
    expert_gain = gfull[1:2, :]
    rf = xf + mixed * lax.rsqrt(jnp.mean(mixed * mixed, axis=-1, keepdims=True) + EPS) * mixed_gain
    resid[...] = rf.astype(BF16)
    ein = (rf * lax.rsqrt(jnp.mean(rf * rf, axis=-1, keepdims=True) + EPS) * expert_gain).astype(BF16)
    for k in range(4):
        xst[k * 16:(k + 1) * 16, :] = ein[:, k * 512:(k + 1) * 512]

    do[...] = mm(oh_s[...], xst[...]).astype(BF16)

    def peer_of(i):
        zz = (z + i // 8 + 2) % 4
        yy = (y + (i // 2) % 4 + 2) % 4
        cc = (c + i % 2) % 2
        return zz * 8 + yy * 2 + cc

    me16 = pl.ds(pl.multiple_of(ep * 16, 16), 16)

    def exchange(src, dst, k):
        def one(i, _):
            p = peer_of(i)
            rows = pl.ds(pl.multiple_of(p * 16, 16), 16)

            @pl.when(p != ep)
            def _():
                pltpu.make_async_remote_copy(
                    src_ref=src.at[rows, :], dst_ref=dst.at[me16, :],
                    send_sem=a2a_s.at[k], recv_sem=a2a_r.at[k],
                    device_id={"ep": p}, device_id_type=pl.DeviceIdType.MESH,
                ).start()
            return 0

        lax.fori_loop(0, 32, one, 0)
        dst[me16, :] = src[me16, :]
        return pltpu.make_async_remote_copy(
            src_ref=src.at[0:496, :], dst_ref=dst.at[0:496, :],
            send_sem=a2a_s.at[k], recv_sem=a2a_r.at[k],
            device_id=partner, device_id_type=pl.DeviceIdType.MESH,
        )

    ex1 = exchange(do, di, 0)
    pltpu.make_async_copy(mem.at[0:6], mem.at[0:6], e_sem).wait()
    ex1.wait_recv()
    yst[...] = mm(perm[...], di[...]).astype(BF16)
    gate = jnp.zeros((128, 512), F32)
    up = jnp.zeros((128, 512), F32)
    for k in range(4):
        rows = yst[k * 128:(k + 1) * 128, :]
        gate = gate + mm(rows, w1[k * 512:(k + 1) * 512, :])
        up = up + mm(rows, w3[k * 512:(k + 1) * 512, :])
    gate = jnp.minimum(gate, LIMIT)
    up = jnp.clip(up, -LIMIT, LIMIT)
    act[...] = ((up + 1.0) * gate * sigmoid(SIG * gate)).astype(BF16)
    for k in range(4):
        blk = mm(act[...], w2[:, k * 512 + 256:(k + 1) * 512])
        bst[k * 128:(k + 1) * 128, :] = blk.astype(BF16)
    zbo[...] = mm(permt[...], bst[...]).astype(BF16)
    ex2 = exchange(zbo, zbi, 1)
    sxs, rxs, x_in = group(rx)
    for d in (2, 1, 3):
        tt = (t + d) % 4
        blk = mm(act[...], w2[:, pl.ds(pl.multiple_of(tt * 512, 512), 256)])
        sx[d - 1] = blk.astype(BF16)
        rcopy(sx.at[d - 1], rx.at[d - 1], xdev(tt), sxs, rxs)
    own_x[...] = mm(act[...], w2[:, pl.ds(pl.multiple_of(t * 512, 512), 256)])
    x_in.wait_recv()
    red = (own_x[...] + jnp.sum(rx[...].astype(F32), axis=0)).astype(BF16)
    for k in range(2):
        rst[k * 128:(k + 1) * 128, :] = red[:, k * 128:(k + 1) * 128]
    zo[...] = mm(permt[:, 0:256], rst[...]).astype(BF16)
    ex3 = exchange(zo, zi, 2)
    ex2.wait_recv()
    cbs[...] = (mm(ohw_hi[...], zbi[...]) + mm(ohw_lo[...], zbi[...])).reshape(4, 16, 256)
    cs_, cr_, c_in = group(cbr)
    for d in (2, 1, 3):
        tt = (t + d) % 4
        rcopy(cbs.at[tt], cbr.at[d - 1], xdev(tt), cs_, cr_)
    ex3.wait_recv()
    half4 = mm(ohw_hi[0:32, :], zi[...]) + mm(ohw_lo[0:32, :], zi[...])
    c_in.wait_recv()
    beta = cbs[t] + jnp.sum(cbr[...], axis=0)
    comb = jnp.concatenate([half4[0:16, :], half4[16:32, :], beta], axis=1)
    sq[t] = jnp.broadcast_to(jnp.sum(comb * comb, axis=-1, keepdims=True), (16, 128))
    sqs, sqr, s_in = group(sq.at[0:3])
    for d in (2, 1, 3):
        rcopy(sq.at[t], sq.at[t], xdev((t + d) % 4), sqs, sqr)
    s_in.wait_recv()
    total = jnp.sum(sq[...], axis=0)[:, 0:1]
    mine = resid[:, own_rows].astype(F32)
    out[...] = (mine + comb * lax.rsqrt(total * (1.0 / 2048.0) + EPS) * og[...]).astype(BF16)
    for cp in ends:
        cp.wait_send()
    ex1.wait_send()
    ex2.wait_send()
    ex3.wait_send()
    assert sems == [N_SEND, N_RECV, N_LOCAL], sems


def shards(
    tokens, mixer_gain, query_weight, key_weight, value_weight, outgate_weight,
    igate_weight, fgate_weight, memory, stabilizer, head_gain, down_weight,
    mixed_gain, expert_gain, routes, route_weights, gate_proj, up_proj, expert_down, output_gain,
):
    V = pltpu.VMEM
    scratch = [
        V((16, 2048), BF16), V((1, 2048), F32),
        V((2, 4, 2, 64, 512), BF16), V((2, 4, 2, 64, 512), BF16),
        V((1, 2048), BF16), V((1, 2048), BF16),
        V((16, 512, 512), F32), V((1, 16), F32), V((1, 512), F32),
        V((4, 4, 2, 64, 512), BF16),
        V((1, 64), F32), V((1, 64), F32), V((4, 4, 2, 8, 128), F32),
        V((4, 512), jnp.int32), V((4, 512), F32),
        V((2048, 512), BF16), V((2048, 512), BF16), V((512, 2048), BF16), V((1, 512), F32),
        V((16, 2048), BF16), V((4, 16, 512), BF16), V((4, 16, 512), BF16), V((4, 16, 512), BF16),
        V((4, 16, 1024), BF16), V((4, 16, 1024), F32), V((4, 16, 1024), BF16), V((4, 16, 1024), F32),
        V((128, 512), F32), V((512, 128), F32), V((16, 512), F32),
        V((4, 16, 2048), BF16), V((8, 2048), F32), V((16, 2048), BF16), V((64, 512), BF16),
        V((512, 64), BF16), V((64, 512), BF16), V((64, 512), BF16),
        V((512, 512), BF16), V((512, 512), BF16),
        V((512, 512), BF16), V((512, 512), BF16), V((512, 512), BF16), V((128, 512), BF16),
        V((3, 128, 256), BF16), V((3, 128, 256), BF16), V((128, 256), F32), V((256, 128), BF16),
        V((512, 128), BF16), V((512, 128), BF16),
        V((512, 256), BF16), V((512, 256), BF16), V((512, 256), BF16),
        V((4, 16, 256), F32), V((3, 16, 256), F32), V((4, 16, 128), F32),
        pltpu.SemaphoreType.DMA((N_SEND,)), pltpu.SemaphoreType.DMA((N_RECV,)),
        pltpu.SemaphoreType.DMA((N_LOCAL,)),
        pltpu.SemaphoreType.DMA((3,)), pltpu.SemaphoreType.DMA((3,)),
    ]
    return pl.pallas_call(
        body,
        out_shape=pltpu.VMEM((16, 512), BF16),
        in_specs=[pl.BlockSpec(memory_space=pl.ANY)] * 20,
        out_specs=pl.BlockSpec(memory_space=pltpu.VMEM),
        scratch_shapes=scratch,
        compiler_params=pltpu.CompilerParams(
            collective_id=0, has_side_effects=True, vmem_limit_bytes=56 * 1024 * 1024
        ),
        name="step",
    )(
        tokens, mixer_gain.reshape(1, 2048), query_weight, key_weight, value_weight, outgate_weight,
        igate_weight, fgate_weight, memory, stabilizer.T, head_gain.reshape(1, 512), down_weight.T,
        mixed_gain.reshape(1, 64), expert_gain.reshape(1, 64), routes.T, route_weights.T,
        gate_proj, up_proj, expert_down, output_gain.reshape(1, 512),
    )


def solution(mesh):
    placed = (
        P("ep", None), P(), P("ep", "tp"), P("ep", "tp"), P("ep", "tp"), P("ep", "tp"),
        P("tp", None), P("tp", None), P("ep", "tp", None, None), P("ep", "tp"), P("tp"),
        P(None, "ep"), P("ep"), P("ep"), P(), P(), P("ep", None, "tp"), P("ep", None, "tp"),
        P("ep", "tp", None), P("tp"),
    )
    return jax.shard_map(
        shards, mesh=mesh, in_specs=placed, out_specs=P("ep", "tp"), check_vma=False
    )
```

```python
import functools
import jax
import jax.numpy as jnp
from jax import lax
from jax.experimental import pallas as pl
from jax.experimental.pallas import tpu as pltpu
from jax.sharding import PartitionSpec as P

EPS = 1e-06
LIMIT = 7.0
SIG = 1.702
F32 = jnp.float32
BF16 = jnp.bfloat16
N_SEND = 15
N_RECV = 20
N_LOCAL = 15


def iota(shape, dim):
    return lax.broadcasted_iota(jnp.int32, shape, dim)


def sigmoid(x):
    return 1.0 / (1.0 + jnp.exp(-x))


def mm(a, b):
    return jnp.dot(a, b, preferred_element_type=F32)


def body(
    tok_h, mixg_h, wq_h, wk_h, wv_h, wo_h, ig_h, fg_h, mem_h, stab_h, hg_h, dw_h,
    mg_h, eg_h, rt_h, rw_h, w1_h, w3_h, w2_h, og_h,
    out,
    tok, mixg, wa, wb, ig, fg, mem, stab, hg, dt, mg, eg, gains, rt, rw, w1, w3, w2, og,
    nrm, na, xa, xb, sa, sb, ra, rb, qpad, qt, read,
    mx, gfull, resid, xst, oh_s, ohw_hi, ohw_lo, perm, permt,
    do, di, yst, act, sx, rx, own_x, rst, zo, zi, bst, zbo, zbi, cbs, cb, sq,
    ss, rs, ls, a2a_s, a2a_r,
):
    ep = lax.axis_index("ep")
    t = lax.axis_index("tp")
    z = ep // 8
    y = (ep // 2) % 4
    c = ep % 2
    partner = {"ep": z * 8 + y * 2 + (1 - c)}

    def zdev(zz):
        return {"ep": zz * 8 + y * 2 + c}

    def ydev(yy):
        return {"ep": z * 8 + yy * 2 + c}

    def xdev(xx):
        return {"tp": xx}

    sems = [0, 0, 0]

    def ssem():
        sems[0] += 1
        return ss.at[sems[0] - 1]

    def rsem():
        sems[1] += 1
        return rs.at[sems[1] - 1]

    def lsem():
        sems[2] += 1
        return ls.at[sems[2] - 1]

    def rcopy(src, dst, dev, s_sem, r_sem, go=True):
        cp = pltpu.make_async_remote_copy(
            src_ref=src, dst_ref=dst, send_sem=s_sem, recv_sem=r_sem,
            device_id=dev, device_id_type=pl.DeviceIdType.MESH,
        )
        if go:
            cp.start()
        return cp

    ends = []

    def group(like):
        s_sem, r_sem = ssem(), rsem()
        whole = rcopy(like, like, partner, s_sem, r_sem, go=False)
        ends.append(whole)
        return s_sem, r_sem, whole

    def lcopy(src, dst, sem=None):
        cp = pltpu.make_async_copy(src, dst, lsem() if sem is None else sem)
        cp.start()
        return cp

    w_sem = lsem()
    l_w = [
        lcopy(wv_h, wa.at[0, z, c], w_sem), lcopy(wo_h, wa.at[1, z, c], w_sem),
        lcopy(wq_h, wb.at[0, y, c], w_sem), lcopy(wk_h, wb.at[1, y, c], w_sem),
    ]
    own_rows = pl.ds(pl.multiple_of(t * 512, 512), 512)
    l_dw = lcopy(dw_h.at[:, own_rows], dt.at[z, y, c])
    l_g = [lcopy(mg_h, mg), lcopy(eg_h, eg)]
    l_tok = lcopy(tok_h, tok)
    l_mixg = lcopy(mixg_h, mixg)
    l_small = [
        lcopy(ig_h, ig), lcopy(fg_h, fg), lcopy(stab_h, stab), lcopy(hg_h, hg),
        lcopy(rt_h, rt), lcopy(rw_h, rw), lcopy(og_h, og),
    ]

    bar = pltpu.get_barrier_semaphore()
    near = [partner]
    for d in (1, 2, 3):
        near += [zdev((z + d) % 4), ydev((y + d) % 4), xdev((t + d) % 4)]
    for dev in near:
        pl.semaphore_signal(bar, inc=1, device_id=dev, device_id_type=pl.DeviceIdType.MESH)

    for cp in l_g:
        cp.wait()
    spread = ((iota((64, 128), 1) & 63) == iota((64, 128), 0)).astype(F32)
    mg128 = jnp.dot(jnp.broadcast_to(mg[...], (8, 64)), spread, precision=lax.Precision.HIGHEST, preferred_element_type=F32)
    eg128 = jnp.dot(jnp.broadcast_to(eg[...], (8, 64)), spread, precision=lax.Precision.HIGHEST, preferred_element_type=F32)
    gains[z, y, c] = jnp.where(iota((8, 128), 0) == 0, mg128, eg128)
    l_dw.wait()
    pltpu.make_async_copy(wa.at[:, 0:1], wa.at[:, 0:1], w_sem).wait()
    pl.semaphore_wait(bar, len(near))

    s1, r1, d1_in = group(dt.at[0:3, 0, 0])
    g1s, g1r, g1_in = group(gains.at[0:3, 0, 0])
    for d in (2, 1, 3):
        zz, yy = (z + d) % 4, (y + d) % 4
        rcopy(dt.at[z, y, c, :, 0:256], dt.at[z, y, c, :, 0:256], zdev(zz), s1, r1)
        rcopy(dt.at[z, y, c, :, 256:512], dt.at[z, y, c, :, 256:512], ydev(yy), s1, r1)
        rcopy(gains.at[z, y, c], gains.at[z, y, c], zdev(zz), g1s, g1r)

    sw, rp, p_in = group(wa)
    a_in, b_in = {}, {}
    for d in (2, 1, 3):
        zz, yy = (z + d) % 4, (y + d) % 4
        a_in[d] = rcopy(wa.at[:, z, c], wa.at[:, z, c], zdev(zz), sw, rsem())
        b_in[d] = rcopy(wb.at[:, y, c], wb.at[:, y, c], ydev(yy), sw, rsem())
    rcopy(wa.at[:, z, c], wa.at[:, z, c], partner, sw, rp)
    rcopy(wb.at[:, y, c], wb.at[:, y, c], partner, sw, rp)
    sf = ssem()
    ends.append(rcopy(wa.at[:, 0:3], wa.at[:, 0:3], partner, sf, rp, go=False))

    l_tok.wait()
    l_mixg.wait()
    x = tok[...].astype(F32)
    ms = jnp.mean(x * x, axis=-1, keepdims=True)
    normed = (x * lax.rsqrt(ms + EPS) * mixg[...]).astype(BF16)
    nrm[...] = normed
    for yy in range(4):
        for zz in range(4):
            na[yy, :, zz * 128:(zz + 1) * 128] = normed[:, zz * 512 + yy * 128:zz * 512 + yy * 128 + 128]
    xa[y] = na[y]
    xb[z] = nrm[:, pl.ds(pl.multiple_of(z * 512, 512), 512)]
    st_, rt_, t_in = group(ra.at[0:3])
    for d in (2, 1, 3):
        zz, yy = (z + d) % 4, (y + d) % 4
        rcopy(na.at[yy], xa.at[y], ydev(yy), st_, rt_)
        rcopy(nrm.at[:, pl.ds(pl.multiple_of(zz * 512, 512), 512)], xb.at[z], zdev(zz), st_, rt_)

    m_sem, e_sem = lsem(), lsem()
    for i in range(8):
        lcopy(mem_h.at[pl.ds(2 * i, 2), 0], mem.at[pl.ds(2 * i, 2)], m_sem)
    for src, dst in ((w1_h, w1), (w3_h, w3), (w2_h, w2)):
        lcopy(src.at[0], dst, e_sem)

    for cp in l_small:
        cp.wait()
    nf = normed.astype(F32)
    log_in = jnp.sum(nf * ig[...].astype(F32), axis=-1, keepdims=True)
    pre_f = jnp.sum(nf * fg[...].astype(F32), axis=-1, keepdims=True)
    log_f = jnp.minimum(pre_f, 0.0) - jnp.log(1.0 + jnp.exp(-jnp.abs(pre_f)))
    eye = iota((16, 16), 0) == iota((16, 16), 1)
    st = jnp.sum(jnp.where(eye, jnp.broadcast_to(stab[...], (16, 16)), 0.0), axis=-1, keepdims=True)
    peak = jnp.maximum(log_f + st, log_in)
    within = jnp.exp(log_in - peak)
    carried = jnp.exp(log_f + st - peak)

    sel = (iota((64, 512), 1) == ep * 16 + (iota((64, 512), 0) & 15))
    col = iota((64, 512), 1)
    cx = jnp.zeros((64, 512), F32)
    wx = jnp.zeros((64, 512), F32)
    for k in range(4):
        r_k = jnp.sum(jnp.where(sel, rt[k:k + 1, :], 0), axis=-1, keepdims=True)
        w_k = jnp.sum(jnp.where(sel, rw[k:k + 1, :], 0.0), axis=-1, keepdims=True)
        hit = ((col >> 4) == r_k).astype(F32)
        cx = cx + hit
        wx = wx + hit * w_k
    r64, c64 = iota((64, 64), 0), iota((64, 64), 1)
    lower = (((r64 >> 4) == (c64 >> 4)) & (c64 < r64)).astype(BF16)
    before = mm(lower, cx.astype(BF16))
    fits = (before == (col & 3).astype(F32)) & (((col >> 2) & 3) == (iota((64, 512), 0) >> 4))
    oh = jnp.where(fits, cx, 0.0)
    oh_s[...] = jnp.transpose(oh).astype(BF16)
    ohw = oh * wx
    hi_part = ohw.astype(BF16)
    ohw_hi[...] = hi_part
    ohw_lo[...] = (ohw - hi_part.astype(F32)).astype(BF16)
    r5, c5 = iota((512, 512), 0), iota((512, 512), 1)
    perm[...] = (c5 == 16 * ((r5 & 127) >> 2) + 4 * (r5 >> 7) + (r5 & 3)).astype(BF16)
    permt[...] = (r5 == 16 * ((c5 & 127) >> 2) + 4 * (c5 >> 7) + (c5 & 3)).astype(BF16)

    d1_in.wait_recv()
    g1_in.wait_recv()
    s2, r2, d2_in = group(dt.at[0:3, :, 0])
    g2s, g2r, g2_in = group(gains.at[0:3, :, 0])
    for d in (2, 1, 3):
        zz, yy = (z + d) % 4, (y + d) % 4
        rcopy(gains.at[:, y, c], gains.at[:, y, c], ydev(yy), g2s, g2r)
        rcopy(dt.at[:, y, c, :, 0:256], dt.at[:, y, c, :, 0:256], ydev(yy), s2, r2)
        rcopy(dt.at[z, :, c, :, 256:512], dt.at[z, :, c, :, 256:512], zdev(zz), s2, r2)

    for d in (1, 3, 2):
        zz, yy = (z + 4 - d) % 4, (y + 4 - d) % 4
        a_in[d].wait_recv()
        rcopy(wa.at[:, zz, c], wa.at[:, zz, c], partner, sf, rp)
        b_in[d].wait_recv()
        rcopy(wb.at[:, yy, c], wb.at[:, yy, c], partner, sf, rp)
    t_in.wait_recv()
    p_in.wait_recv()

    ax = xa[...].reshape(64, 512)
    bx = xb[...].reshape(64, 512)
    sq_, rq_, q_in = group(dt.at[0:3, 0, 0])
    sv_, rv_, v_in = group(ra.at[0:3])
    for k in range(2):
        cols = pl.ds(k * 512, 512)
        sb[:, :, cols] = mm(bx, wb[k].reshape(512, 512)).reshape(4, 16, 512)
        for d in (2, 1, 3):
            zz = (z + d) % 4
            rcopy(sb.at[zz, :, cols], rb.at[z, :, cols], zdev(zz), sq_, rq_)
    for k in range(2):
        cols = pl.ds(k * 512, 512)
        sa[:, :, cols] = mm(ax, wa[k].reshape(512, 512)).astype(BF16).reshape(4, 16, 512)
        for d in (2, 1, 3):
            yy = (y + d) % 4
            rcopy(sa.at[yy, :, cols], ra.at[y, :, cols], ydev(yy), sv_, rv_)
    ra[y] = sa[y]
    rb[z] = sb[z]

    d2_in.wait_recv()
    g2_in.wait_recv()
    s3, r3, d3_in = group(dt.at[:, :, 0])
    g3s, g3r, g3_in = group(gains.at[:, :, 0])
    rcopy(dt.at[:, :, c], dt.at[:, :, c], partner, s3, r3)
    rcopy(gains.at[:, :, c], gains.at[:, :, c], partner, g3s, g3r)

    q_in.wait_recv()
    v_in.wait_recv()
    qk = jnp.sum(rb[...], axis=0).astype(BF16).astype(F32)
    q = qk[:, 0:512] * (512.0 ** -0.5)
    key = qk[:, 512:]
    vo = jnp.sum(ra[...].astype(F32), axis=0)
    val = vo[:, 0:512]
    og_pre = vo[:, 512:]
    qpad[0:16, :] = q
    qpad[16:128, :] = jnp.zeros((112, 512), F32)
    qt[...] = jnp.transpose(qpad[...])
    pltpu.make_async_copy(mem, mem, m_sem).wait()
    for n in range(16):
        qcol = qt[:, n:n + 1]
        read[n:n + 1, :] = jnp.sum(qcol * mem[n], axis=0, keepdims=True)

    score = jnp.sum(q * key, axis=-1, keepdims=True) * within
    rd = score * val + carried * read[...]
    mean = jnp.mean(rd, axis=-1, keepdims=True)
    cen = rd - mean
    var = jnp.mean(cen * cen, axis=-1, keepdims=True)
    gated = (cen * lax.rsqrt(var + EPS) * hg[...] * sigmoid(og_pre)).astype(BF16)
    d3_in.wait_recv()
    g3_in.wait_recv()
    sm, rm, m_in = group(mx.at[0:3])
    for k in range(4):
        cols = pl.ds(k * 512, 512)
        part = lax.dot_general(
            gated, dt[k].reshape(512, 512), (((1,), (1,)), ((), ())), preferred_element_type=F32
        )
        mx[t, :, cols] = part.astype(BF16)
        for d in (2, 1, 3):
            rcopy(mx.at[t, :, cols], mx.at[t, :, cols], xdev((t + d) % 4), sm, rm)
    low = iota((1, 128), 1) < 64
    for zz in range(4):
        for yy in range(4):
            at = zz * 512 + yy * 128
            g0, g1 = gains[zz, yy, 0], gains[zz, yy, 1]
            gfull[:, at:at + 128] = jnp.where(low, g0, g1)
    m_in.wait_recv()
    mixed = jnp.sum(mx[...].astype(F32), axis=0)
    xf = tok[...].astype(F32)
    mixed_gain = gfull[0:1, :]
    expert_gain = gfull[1:2, :]
    rf = xf + mixed * lax.rsqrt(jnp.mean(mixed * mixed, axis=-1, keepdims=True) + EPS) * mixed_gain
    resid[...] = rf.astype(BF16)
    ein = (rf * lax.rsqrt(jnp.mean(rf * rf, axis=-1, keepdims=True) + EPS) * expert_gain).astype(BF16)
    for k in range(4):
        xst[k * 16:(k + 1) * 16, :] = ein[:, k * 512:(k + 1) * 512]

    do[...] = mm(oh_s[...], xst[...]).astype(BF16)

    def peer_of(i):
        zz = (z + i // 8 + 2) % 4
        yy = (y + (i // 2) % 4 + 2) % 4
        cc = (c + i % 2) % 2
        return zz * 8 + yy * 2 + cc

    me16 = pl.ds(pl.multiple_of(ep * 16, 16), 16)

    def exchange(src, dst, k):
        def one(i, _):
            p = peer_of(i)
            rows = pl.ds(pl.multiple_of(p * 16, 16), 16)

            @pl.when(p != ep)
            def _():
                pltpu.make_async_remote_copy(
                    src_ref=src.at[rows, :], dst_ref=dst.at[me16, :],
                    send_sem=a2a_s.at[k], recv_sem=a2a_r.at[k],
                    device_id={"ep": p}, device_id_type=pl.DeviceIdType.MESH,
                ).start()
            return 0

        lax.fori_loop(0, 32, one, 0)
        dst[me16, :] = src[me16, :]
        return pltpu.make_async_remote_copy(
            src_ref=src.at[0:496, :], dst_ref=dst.at[0:496, :],
            send_sem=a2a_s.at[k], recv_sem=a2a_r.at[k],
            device_id=partner, device_id_type=pl.DeviceIdType.MESH,
        )

    ex1 = exchange(do, di, 0)
    pltpu.make_async_copy(mem.at[0:6], mem.at[0:6], e_sem).wait()
    ex1.wait_recv()
    yst[...] = mm(perm[...], di[...]).astype(BF16)
    gate = jnp.zeros((128, 512), F32)
    up = jnp.zeros((128, 512), F32)
    for k in range(4):
        rows = yst[k * 128:(k + 1) * 128, :]
        gate = gate + mm(rows, w1[k * 512:(k + 1) * 512, :])
        up = up + mm(rows, w3[k * 512:(k + 1) * 512, :])
    gate = jnp.minimum(gate, LIMIT)
    up = jnp.clip(up, -LIMIT, LIMIT)
    act[...] = ((up + 1.0) * gate * sigmoid(SIG * gate)).astype(BF16)
    sxs, rxs, x_in = group(rx)
    for d in (2, 1, 3):
        tt = (t + d) % 4
        blk = mm(act[...], w2[:, pl.ds(pl.multiple_of(tt * 512, 512), 256)])
        sx[d - 1] = blk.astype(BF16)
        rcopy(sx.at[d - 1], rx.at[d - 1], xdev(tt), sxs, rxs)
    own_x[...] = mm(act[...], w2[:, pl.ds(pl.multiple_of(t * 512, 512), 256)])
    for k in range(4):
        blk = mm(act[...], w2[:, k * 512 + 256:(k + 1) * 512])
        bst[k * 128:(k + 1) * 128, :] = blk.astype(BF16)
    zbo[...] = mm(permt[...], bst[...]).astype(BF16)
    ex2 = exchange(zbo, zbi, 1)
    x_in.wait_recv()
    red = (own_x[...] + jnp.sum(rx[...].astype(F32), axis=0)).astype(BF16)
    for k in range(2):
        rst[k * 128:(k + 1) * 128, :] = red[:, k * 128:(k + 1) * 128]
    zo[...] = mm(permt[:, 0:256], rst[...]).astype(BF16)
    ex3 = exchange(zo, zi, 2)
    ex2.wait_recv()
    cb[t] = (mm(ohw_hi[...], zbi[...]) + mm(ohw_lo[...], zbi[...])).astype(BF16).reshape(4, 16, 256)
    cs_, cr_, c_in = group(cb.at[0:3])
    for d in (2, 1, 3):
        rcopy(cb.at[t], cb.at[t], xdev((t + d) % 4), cs_, cr_)
    ex3.wait_recv()
    half4 = mm(ohw_hi[0:32, :], zi[...]) + mm(ohw_lo[0:32, :], zi[...])
    alpha = jnp.concatenate([half4[0:16, :], half4[16:32, :]], axis=1)
    sq[t] = jnp.broadcast_to(jnp.sum(alpha * alpha, axis=-1, keepdims=True), (16, 128))
    sqs, sqr, s_in = group(sq.at[0:3])
    for d in (2, 1, 3):
        rcopy(sq.at[t], sq.at[t], xdev((t + d) % 4), sqs, sqr)
    c_in.wait_recv()
    whole_b = jnp.sum(cb[...].astype(F32), axis=0)
    cbs[...] = whole_b
    squares_b = jnp.sum(jnp.sum(whole_b * whole_b, axis=0), axis=-1, keepdims=True)
    comb = jnp.concatenate([alpha, cbs[t]], axis=1)
    s_in.wait_recv()
    total = jnp.sum(sq[...], axis=0)[:, 0:1] + squares_b
    mine = resid[:, own_rows].astype(F32)
    out[...] = (mine + comb * lax.rsqrt(total * (1.0 / 2048.0) + EPS) * og[...]).astype(BF16)
    for cp in ends:
        cp.wait_send()
    ex1.wait_send()
    ex2.wait_send()
    ex3.wait_send()
    assert sems == [N_SEND, N_RECV, N_LOCAL], sems


def shards(
    tokens, mixer_gain, query_weight, key_weight, value_weight, outgate_weight,
    igate_weight, fgate_weight, memory, stabilizer, head_gain, down_weight,
    mixed_gain, expert_gain, routes, route_weights, gate_proj, up_proj, expert_down, output_gain,
):
    V = pltpu.VMEM
    scratch = [
        V((16, 2048), BF16), V((1, 2048), F32),
        V((2, 4, 2, 64, 512), BF16), V((2, 4, 2, 64, 512), BF16),
        V((1, 2048), BF16), V((1, 2048), BF16),
        V((16, 512, 512), F32), V((1, 16), F32), V((1, 512), F32),
        V((4, 4, 2, 64, 512), BF16),
        V((1, 64), F32), V((1, 64), F32), V((4, 4, 2, 8, 128), F32),
        V((4, 512), jnp.int32), V((4, 512), F32),
        V((2048, 512), BF16), V((2048, 512), BF16), V((512, 2048), BF16), V((1, 512), F32),
        V((16, 2048), BF16), V((4, 16, 512), BF16), V((4, 16, 512), BF16), V((4, 16, 512), BF16),
        V((4, 16, 1024), BF16), V((4, 16, 1024), F32), V((4, 16, 1024), BF16), V((4, 16, 1024), F32),
        V((128, 512), F32), V((512, 128), F32), V((16, 512), F32),
        V((4, 16, 2048), BF16), V((8, 2048), F32), V((16, 2048), BF16), V((64, 512), BF16),
        V((512, 64), BF16), V((64, 512), BF16), V((64, 512), BF16),
        V((512, 512), BF16), V((512, 512), BF16),
        V((512, 512), BF16), V((512, 512), BF16), V((512, 512), BF16), V((128, 512), BF16),
        V((3, 128, 256), BF16), V((3, 128, 256), BF16), V((128, 256), F32), V((256, 128), BF16),
        V((512, 128), BF16), V((512, 128), BF16),
        V((512, 256), BF16), V((512, 256), BF16), V((512, 256), BF16),
        V((4, 16, 256), F32), V((4, 4, 16, 256), BF16), V((4, 16, 128), F32),
        pltpu.SemaphoreType.DMA((N_SEND,)), pltpu.SemaphoreType.DMA((N_RECV,)),
        pltpu.SemaphoreType.DMA((N_LOCAL,)),
        pltpu.SemaphoreType.DMA((3,)), pltpu.SemaphoreType.DMA((3,)),
    ]
    return pl.pallas_call(
        body,
        out_shape=pltpu.VMEM((16, 512), BF16),
        in_specs=[pl.BlockSpec(memory_space=pl.ANY)] * 20,
        out_specs=pl.BlockSpec(memory_space=pltpu.VMEM),
        scratch_shapes=scratch,
        compiler_params=pltpu.CompilerParams(
            collective_id=0, has_side_effects=True, vmem_limit_bytes=56 * 1024 * 1024
        ),
        name="step",
    )(
        tokens, mixer_gain.reshape(1, 2048), query_weight, key_weight, value_weight, outgate_weight,
        igate_weight, fgate_weight, memory, stabilizer.T, head_gain.reshape(1, 512), down_weight.T,
        mixed_gain.reshape(1, 64), expert_gain.reshape(1, 64), routes.T, route_weights.T,
        gate_proj, up_proj, expert_down, output_gain.reshape(1, 512),
    )


def solution(mesh):
    placed = (
        P("ep", None), P(), P("ep", "tp"), P("ep", "tp"), P("ep", "tp"), P("ep", "tp"),
        P("tp", None), P("tp", None), P("ep", "tp", None, None), P("ep", "tp"), P("tp"),
        P(None, "ep"), P("ep"), P("ep"), P(), P(), P("ep", None, "tp"), P("ep", None, "tp"),
        P("ep", "tp", None), P("tp"),
    )
    return jax.shard_map(
        shards, mesh=mesh, in_specs=placed, out_specs=P("ep", "tp"), check_vma=False
    )
```
